512 devices in a mesh: ep: 32 (over z, core), tp: 16 (over y, x).
Axes of the slice: x: 4, y: 4, z: 16, core: 2. Of those that a mesh axis runs over, the one named last changes fastest.
Arguments:
- query_proj: bfloat16 [16384, 1024], P('ep', 'tp'), may hold values from -6 to 6
- key_proj: bfloat16 [16384, 256], P('ep'), may hold values from -6 to 6
- value_proj: bfloat16 [16384, 256], P('ep'), may hold values from -24 to 24
- sink_logit: float32 [16], P('tp'), may hold values from 2 to 6
- out_weight: bfloat16 [1024, 2048], P(None, 'tp'), may hold values from -0.1875 to 0.1875
- expert_input: bfloat16 [8192, 2048], P('ep'), may hold values from -6 to 6
- norm_gain: float32 [2048], replicated, may hold values from 0.1 to 1.9
- routes: int32 [8192, 2], P('ep'), may hold values from 0 to 31, as said below
- route_weights: float32 [8192, 2], P('ep'), may hold values from 0.2 to 1
- gate_weight: bfloat16 [32, 2048, 4096], P('ep', None, 'tp'), may hold values from -0.125 to 0.125
- up_weight: bfloat16 [32, 2048, 4096], P('ep', None, 'tp'), may hold values from -0.125 to 0.125
- down_weight: bfloat16 [32, 4096, 2048], P('ep', 'tp'), may hold values from -0.09375 to 0.09375
Outputs:
- mixer_out: bfloat16 [16384, 2048], P('ep', 'tp')
- expert_out: bfloat16 [8192, 2048], P('ep', 'tp')
The draws below stay inside these ranges and needn't reach their ends.
Inputs may be any that keep to these rules, and one draw needn't show every extreme that they name: `routes`: experts form 4 groups of consecutive numbers of equal size. Each row names 2 different experts of one group. In each aligned block of 256 rows no expert is named by more than 32 rows, and in every block some expert is named by exactly 32 rows.
All inputs are finite; a program needn't handle non-finite values.
Results may differ from the reference program's by a relative error of at most 0.017.
Values may be sent and summed in bfloat16 or wider, within the bound.
A program may use at most 64 MiB of HBM per device.

```python
import jax
import jax.numpy as jnp
from jax import lax

D = 2048
HEADS = 16
KV_HEADS = 4
HEAD_DIM = 64
HALF_WIN = 128
ROWS_B = 256
TOK_A = 16384
TOK_B = 8192
EXPERTS = 32
GROUPS = 4
TOP_K = 2
EXP_HID = 4096
CAP = 32
N_TP = 16


def drawn_pair(key):
    base_key = jax.random.fold_in(key, 7)
    key_rows = jax.random.normal(jax.random.fold_in(base_key, 1), (TOK_A, KV_HEADS * HEAD_DIM), jnp.float32)
    query_rows = jax.random.normal(jax.random.fold_in(base_key, 2), (TOK_A, HEADS * HEAD_DIM), jnp.float32)
    return (jnp.clip(query_rows, -6.0, 6.0), jnp.clip(key_rows, -6.0, 6.0))


def draw_query_proj(key, part):
    return drawn_pair(key)[0].astype(jnp.bfloat16)


def draw_key_proj(key, part):
    return drawn_pair(key)[1].astype(jnp.bfloat16)


def draw_routes(key, part):
    per_group = EXPERTS // GROUPS
    block_count = TOK_B // ROWS_B
    base_key = jax.random.fold_in(key, 31)
    busy_group = jax.random.randint(jax.random.fold_in(base_key, 1), (block_count, 1), 0, GROUPS)
    other_step = jax.random.randint(jax.random.fold_in(base_key, 2), (block_count, ROWS_B), 1, GROUPS)
    order_keys = jax.random.split(jax.random.fold_in(base_key, 3), block_count)
    row_order = jax.vmap(lambda sub_key: jax.random.permutation(sub_key, ROWS_B))(order_keys)
    in_busy = row_order < ROWS_B // 2
    group_ids = jnp.where(in_busy, busy_group, (busy_group + other_step) % GROUPS)
    onehot = (group_ids[:, :, None] == jnp.arange(GROUPS, dtype=jnp.int32)[None, None, :]).astype(jnp.int32)
    group_rank = jnp.sum((jnp.cumsum(onehot, axis=1) - onehot) * onehot, axis=2)
    offsets = jax.random.randint(jax.random.fold_in(base_key, 4), (block_count, GROUPS), 0, per_group)
    shifts = jax.random.randint(jax.random.fold_in(base_key, 5), (block_count, GROUPS), 1, per_group)
    offset_row = jnp.take_along_axis(offsets, group_ids, axis=1)
    shift_row = jnp.take_along_axis(shifts, group_ids, axis=1)
    first_pick = (group_rank + offset_row) % per_group
    second_pick = (group_rank + offset_row + shift_row) % per_group
    chosen = group_ids[:, :, None] * per_group + jnp.stack([first_pick, second_pick], axis=-1)
    return chosen.reshape(TOK_B, TOP_K).astype(jnp.int32)


def block_levels(stream_key, dims, cuts, low, top_value):
    loudness = 1.0
    for axis_at, blocks in cuts:
        draws = jax.random.uniform(jax.random.fold_in(jax.random.fold_in(stream_key, 6), axis_at), (blocks,), jnp.float32, low / len(cuts), top_value / len(cuts))
        loudness = loudness * jnp.repeat(jnp.exp(draws), dims[axis_at] // blocks).reshape((-1,) + (1,) * (len(dims) - 1 - axis_at))
    return loudness


def centred(own_key, extent, spread, bound, cuts=(), held_as=jnp.bfloat16):
    result = spread * jax.random.normal(own_key, extent, jnp.float32)
    if cuts:
        result = result * block_levels(own_key, extent, cuts, -0.22, 0.18)
    return jnp.clip(result, -bound, bound).astype(held_as)


def setup_inputs(seed: int = 0) -> dict:
    splits = jax.random.split(jax.random.key(seed), 13)
    query_proj = draw_query_proj(jax.random.fold_in(splits[12], 71), 0)
    key_proj = draw_key_proj(jax.random.fold_in(splits[12], 71), 0)
    value_proj = centred(splits[2], (TOK_A, KV_HEADS * HEAD_DIM), 4.0, 24.0, ((0, 32),))
    sink_logit = jnp.clip(2.0 + 4.0 * jax.random.uniform(splits[3], (HEADS,), jnp.float32) ** block_levels(splits[3], (HEADS,), ((0, 16),), -0.2, 0.2), 2.0, 6.0)
    out_weight = centred(splits[4], (HEADS * HEAD_DIM, D), (HEADS * HEAD_DIM) ** -0.5, 0.1875, ((1, 16),))
    expert_input = centred(splits[5], (TOK_B, D), 1.0, 6.0, ((0, 32),))
    norm_gain = jnp.clip(1.0 + 0.18 * jax.random.normal(splits[6], (D,), jnp.float32), 0.1, 1.9)
    routes = draw_routes(jax.random.fold_in(splits[12], 71), 0)
    route_weights = jnp.clip(0.2 + 0.8 * jax.random.uniform(splits[8], (TOK_B, TOP_K), jnp.float32) ** block_levels(splits[8], (TOK_B, TOP_K), ((0, 32),), -0.2, 0.2), 0.2, 1.0)
    gate_weight = centred(splits[9], (EXPERTS, D, EXP_HID), D ** -0.5, 0.125, ((0, 32), (2, 16)))
    up_weight = centred(splits[10], (EXPERTS, D, EXP_HID), D ** -0.5, 0.125, ((0, 32), (2, 16)))
    down_weight = centred(splits[11], (EXPERTS, EXP_HID, D), EXP_HID ** -0.5, 0.09375, ((0, 32), (1, 16)))
    return dict(query_proj=query_proj, key_proj=key_proj, value_proj=value_proj, sink_logit=sink_logit, out_weight=out_weight, expert_input=expert_input, norm_gain=norm_gain, routes=routes, route_weights=route_weights, gate_weight=gate_weight, up_weight=up_weight, down_weight=down_weight)


NORM_EPS = 1e-06
ROPE_BASE = 10000.0
NEG_BIG = -1e+30

def rotate(features, position_start):
    count = features.shape[0]
    half_dim = features.shape[-1] // 2
    inverse_freq = 1.0 / ROPE_BASE ** (jnp.arange(half_dim, dtype=jnp.float32) * 2.0 / features.shape[-1])
    position = (jnp.arange(count, dtype=jnp.int32) + position_start).astype(jnp.float32)
    angles = position[:, None] * inverse_freq[None, :]
    cosine = jnp.cos(angles)[:, None, :]
    sine_part = jnp.sin(angles)[:, None, :]
    lower_half = features[..., :half_dim]
    upper_half = features[..., half_dim:]
    return jnp.concatenate([lower_half * cosine - upper_half * sine_part, upper_half * cosine + lower_half * sine_part], axis=-1)

def attention_ref(query_proj, key_proj, value_proj, sink_logit):
    seq_total = query_proj.shape[0]
    per_kv = HEADS // KV_HEADS
    rot_q = rotate(query_proj.reshape(seq_total, HEADS, HEAD_DIM).astype(jnp.float32), 0).astype(jnp.bfloat16)
    rot_k = rotate(key_proj.reshape(seq_total, KV_HEADS, HEAD_DIM).astype(jnp.float32), 0).astype(jnp.bfloat16)
    padding = ((HALF_WIN, HALF_WIN), (0, 0), (0, 0))
    padded_k = jnp.pad(rot_k, padding)
    padded_v = jnp.pad(value_proj.reshape(seq_total, KV_HEADS, HEAD_DIM), padding)
    grouped_sink = sink_logit.reshape(KV_HEADS, per_kv)
    block_rows = min(512, seq_total)
    key_rows = block_rows + 2 * HALF_WIN

    def one_block(block_index):
        start_row = block_index * block_rows
        query_block = lax.dynamic_slice_in_dim(rot_q, start_row, block_rows, 0).reshape(block_rows, KV_HEADS, per_kv, HEAD_DIM).astype(jnp.float32)
        key_block = lax.dynamic_slice_in_dim(padded_k, start_row, key_rows, 0).astype(jnp.float32)
        value_block = lax.dynamic_slice_in_dim(padded_v, start_row, key_rows, 0).astype(jnp.float32)
        scores = jnp.einsum('qngd,knd->ngqk', query_block, key_block) * HEAD_DIM ** (-0.5)
        key_offset = jnp.arange(key_rows, dtype=jnp.int32) - HALF_WIN
        key_gap = key_offset[None, :] - jnp.arange(block_rows, dtype=jnp.int32)[:, None]
        global_key = start_row + key_offset
        allowed = (jnp.abs(key_gap) <= HALF_WIN) & (global_key >= 0)[None, :] & (global_key < seq_total)[None, :]
        scores = jnp.where(allowed[None, None], scores, NEG_BIG)
        row_peak = jnp.maximum(lax.optimization_barrier(jnp.max(scores, axis=-1)), grouped_sink[:, :, None])
        lifted = jnp.exp(scores - row_peak[..., None])
        norm_total = lax.optimization_barrier(jnp.sum(lifted, axis=-1)) + jnp.exp(grouped_sink[:, :, None] - row_peak)
        probs = (lifted / norm_total[..., None]).astype(jnp.bfloat16)
        weighted = jnp.einsum('ngqk,knd->qngd', probs.astype(jnp.float32), value_block)
        return weighted.astype(jnp.bfloat16).reshape(block_rows, HEADS * HEAD_DIM)
    blocks = lax.map(one_block, jnp.arange(seq_total // block_rows, dtype=jnp.int32))
    return blocks.reshape(seq_total, HEADS * HEAD_DIM)

def experts_ref(expert_input, norm_gain, routes, route_weights, gate_weight, up_weight, down_weight):
    widened = expert_input.astype(jnp.float32)
    normed = (widened * lax.rsqrt(lax.optimization_barrier(jnp.mean(widened * widened, axis=1, keepdims=True)) + NORM_EPS) * norm_gain).astype(jnp.bfloat16)
    block_count = TOK_B // ROWS_B
    flat_routes = routes.reshape(block_count, ROWS_B * TOP_K)
    onehot = (flat_routes[:, :, None] == jnp.arange(EXPERTS, dtype=jnp.int32)[None, None, :]).astype(jnp.int32)
    slot_rank = lax.optimization_barrier(jnp.sum((jnp.cumsum(onehot, axis=1) - onehot) * onehot, axis=2))
    row_index = (jnp.arange(TOK_B * TOP_K, dtype=jnp.int32) // TOP_K).reshape(block_count, ROWS_B * TOP_K)
    block_index = jnp.broadcast_to(jnp.arange(block_count, dtype=jnp.int32)[:, None], flat_routes.shape)
    table = jnp.zeros((EXPERTS, block_count, CAP), jnp.int32).at[flat_routes, block_index, slot_rank].set(row_index)
    span_units = EXP_HID // N_TP

    def one_expert(operands):
        rows_table, gate_x, up_x, down_x = operands
        gathered = normed[rows_table.reshape(-1)]
        gate_sum = jnp.dot(gathered, gate_x, preferred_element_type=jnp.float32)
        up_sum = jnp.dot(gathered, up_x, preferred_element_type=jnp.float32)
        hidden = (jax.nn.silu(gate_sum) * up_sum).astype(jnp.bfloat16)
        slot_total = hidden.shape[0]
        parts = jnp.einsum('snh,nhd->nsd', hidden.reshape(slot_total, N_TP, span_units).astype(jnp.float32), down_x.reshape(N_TP, span_units, D).astype(jnp.float32)).astype(jnp.bfloat16)
        return lax.optimization_barrier(jnp.sum(parts.astype(jnp.float32), axis=0)).astype(jnp.bfloat16)
    results = lax.map(one_expert, (table, gate_weight, up_weight, down_weight))
    picked = results[flat_routes, block_index * CAP + slot_rank]
    picked = picked.reshape(TOK_B, TOP_K, D).astype(jnp.float32)
    return lax.optimization_barrier(jnp.sum(picked * route_weights[:, :, None], axis=1)).astype(jnp.bfloat16)

def reference(query_proj, key_proj, value_proj, sink_logit, out_weight, expert_input, norm_gain, routes, route_weights, gate_weight, up_weight, down_weight):
    attended = attention_ref(query_proj, key_proj, value_proj, sink_logit)
    mixer_out = jnp.dot(attended, out_weight, preferred_element_type=jnp.float32).astype(jnp.bfloat16)
    expert_out = experts_ref(expert_input, norm_gain, routes, route_weights, gate_weight, up_weight, down_weight)
    return (mixer_out, expert_out)
```

```python
import functools

import jax
import jax.numpy as jnp
from jax import lax
from jax.experimental import pallas as pl
from jax.experimental.pallas import tpu as pltpu
from jax.sharding import Mesh
from jax.sharding import PartitionSpec as P

HEADS = 16
KV_HEADS = 4
HEAD_DIM = 64
HALF_WIN = 128
GROUPS = 4
NORM_EPS = 1e-06
ROPE_BASE = 10000.0
NEG_BIG = -1e30
TP = ("tp_0", "tp_1")
SIDE = 4
LANES = 128
PER_UNIT = 4
BF16 = jnp.bfloat16
F32 = jnp.float32
MESH = pl.DeviceIdType.MESH


def padded(block, width):
    count = lax.axis_size("ep")
    forward = [(i, i + 1) for i in range(count - 1)]
    backward = [(target, source) for source, target in forward]
    low = lax.ppermute(block[:, block.shape[1] - width :], "ep", forward)
    high = lax.ppermute(block[:, :width], "ep", backward)
    return jnp.concatenate([low, block, high], axis=1)


def rotate(features, position_start):
    count = features.shape[0]
    half_dim = features.shape[-1] // 2
    inverse_freq = 1.0 / ROPE_BASE ** (
        jnp.arange(half_dim, dtype=F32) * 2.0 / features.shape[-1]
    )
    position = (jnp.arange(count, dtype=jnp.int32) + position_start).astype(F32)
    angles = position[:, None] * inverse_freq[None, :]
    cosine = jnp.cos(angles)
    sine_part = jnp.sin(angles)
    lower_half = features[..., :half_dim]
    upper_half = features[..., half_dim:]
    return jnp.concatenate(
        [
            lower_half * cosine - upper_half * sine_part,
            upper_half * cosine + lower_half * sine_part,
        ],
        axis=-1,
    )


def attend(query_proj, key_proj, value_proj, sink_logit):
    row_count = query_proj.shape[0]
    offset = lax.axis_index("ep") * row_count
    seq_total = row_count * lax.axis_size("ep")
    first_kv = lax.axis_index(TP) // (HEADS // KV_HEADS)
    own_keys = lax.dynamic_slice_in_dim(key_proj, first_kv * HEAD_DIM, HEAD_DIM, 1)
    own_values = lax.dynamic_slice_in_dim(value_proj, first_kv * HEAD_DIM, HEAD_DIM, 1)
    rot_q = rotate(query_proj.astype(F32), offset).astype(BF16)
    rot_k = rotate(own_keys.astype(F32), offset).astype(BF16)
    extended = padded(jnp.stack([rot_k, own_values]), HALF_WIN)
    key_rows = row_count + 2 * HALF_WIN
    key_offset = jnp.arange(key_rows, dtype=jnp.int32) - HALF_WIN
    key_gap = key_offset[None, :] - jnp.arange(row_count, dtype=jnp.int32)[:, None]
    scores = jnp.einsum("qd,kd->qk", rot_q, extended[0], preferred_element_type=F32)
    scores = scores * HEAD_DIM ** (-0.5)
    global_key = offset + key_offset
    allowed = (
        (jnp.abs(key_gap) <= HALF_WIN)
        & (global_key >= 0)[None, :]
        & (global_key < seq_total)[None, :]
    )
    scores = jnp.where(allowed, scores, NEG_BIG)
    row_peak = jnp.maximum(jnp.max(scores, axis=-1), sink_logit[0])
    lifted = jnp.exp(scores - row_peak[:, None])
    norm_total = jnp.sum(lifted, axis=-1) + jnp.exp(sink_logit[0] - row_peak)
    probs = (lifted / norm_total[:, None]).astype(BF16)
    weighted = jnp.einsum("qk,kd->dq", probs, extended[1], preferred_element_type=F32)
    return weighted.astype(BF16)


def exchange_kernel(
    units,
    out_ref,
    att_ref,
    wg_hbm,
    wu_hbm,
    wd_hbm,
    ret_ref,
    atts_ref,
    rows,
    terms,
    transit,
    from_b,
    part,
    from_a,
    result,
    wg,
    wu,
    wd,
    w_sem,
    z_send,
    z_recv,
    ret_send,
    ret_recv,
    ag_send,
    ag_recv,
    rs_send,
    rs_recv,
    att_send,
    att_recv,
):
    ep = lax.axis_index("ep")
    yi = lax.axis_index("tp_0")
    xi = lax.axis_index("tp_1")
    senders = units * PER_UNIT
    chips = senders // 2
    zi = ep // 2
    ci = ep % 2
    cap = out_ref.shape[1]

    def ep_plus(step, flip):
        return ((zi + step) % chips) * 2 + (ci + flip) % 2

    def along_a(par, k):
        return {"tp_0": (yi + k * par) % SIDE, "tp_1": (xi + k * (1 - par)) % SIDE}

    def along_b(par, k):
        return {"tp_0": (yi + k * (1 - par)) % SIDE, "tp_1": (xi + k * par) % SIDE}

    def own_ab(par):
        return xi * (1 - par) + yi * par, yi * (1 - par) + xi * par

    def remote(src, dst, ssem, rsem, dev):
        return pltpu.make_async_remote_copy(
            src_ref=src,
            dst_ref=dst,
            send_sem=ssem,
            recv_sem=rsem,
            device_id=dev,
            device_id_type=MESH,
        )

    loads = [
        pltpu.make_async_copy(src, dst, w_sem.at[i])
        for i, (src, dst) in enumerate(((wg_hbm, wg), (wu_hbm, wu), (wd_hbm, wd)))
    ]
    for load in loads:
        load.start()

    barrier = pltpu.get_barrier_semaphore()
    for j in range(1, senders):
        pl.semaphore_signal(
            barrier, inc=1, device_id={"ep": ep_plus(j // 2, j % 2)}, device_id_type=MESH
        )
    for par in range(2):
        for k in range(1, SIDE):
            pl.semaphore_signal(
                barrier, inc=1, device_id=along_a(par, k), device_id_type=MESH
            )
    pl.semaphore_wait(barrier, senders - 1 + 2 * (SIDE - 1))

    def z_copy(j):
        u, i = j // PER_UNIT, j % PER_UNIT
        a, b = own_ab(u % 2)
        dest = ep_plus(j // 2, j % 2)
        return remote(
            out_ref.at[dest],
            rows.at[u, b, a, pl.ds(i * cap, cap), :],
            z_send.at[j],
            z_recv.at[j],
            {"ep": dest},
        )

    a0, b0 = own_ab(0)
    rows[0, b0, a0, 0:cap, :] = out_ref[ep]
    for j in range(1, senders):
        z_copy(j).start()

    def gather_a(buf, u, par, ssem, rsem):
        a, b = own_ab(par)
        return [
            remote(
                buf.at[u, b, a], buf.at[u, b, a], ssem.at[u, k - 1], rsem.at[u, k - 1], along_a(par, k)
            )
            for k in range(1, SIDE)
        ]

    def gather_a_in(buf, u, par, ssem, rsem):
        a, b = own_ab(par)
        return [
            remote(
                buf.at[u, b, a],
                buf.at[u, b, (a + SIDE - k) % SIDE],
                ssem.at[u, k - 1],
                rsem.at[u, k - 1],
                along_a(par, k),
            )
            for k in range(1, SIDE)
        ]

    def gather_b(buf, u, par, ssem, rsem, back):
        a, b = own_ab(par)
        out = []
        for i, k in enumerate((1, SIDE - 1)):
            at = (b + SIDE - k) % SIDE if back else b
            out.append(
                remote(
                    buf.at[u, b], buf.at[u, at], ssem.at[u, 3 + i], rsem.at[u, 3 + i], along_b(par, k)
                )
            )
        return out

    def gather_c(buf, u, par, ssem, rsem, back):
        a, b = own_ab(par)
        out = []
        for i, k in enumerate((1, SIDE - 1)):
            held = (b + SIDE - k) % SIDE
            at = (b + 2) % SIDE if back else held
            half = pl.ds(2 * i, 2)
            out.append(
                remote(
                    buf.at[u, held, half],
                    buf.at[u, at, half],
                    ssem.at[u, 5 + i],
                    rsem.at[u, 5 + i],
                    along_b(par, k),
                )
            )
        return out

    def start(copies):
        for copy in copies:
            copy.start()

    def arrive(copies):
        for copy in copies:
            copy.wait_recv()

    def sent(copies):
        for copy in copies:
            copy.wait_send()

    rows_sems = (ag_send, ag_recv)
    att_sems = (att_send, att_recv)

    for h in range(2):
        a, b = own_ab(h)
        atts_ref[h, b, a] = att_ref[h]
    for h in range(2):
        a, b = own_ab(h)
        start(gather_a(atts_ref, h, h, *att_sems))

    def reduce_1(u, par, back):
        a, b = own_ab(par)
        out = []
        for i, k in enumerate((1, SIDE - 1)):
            half, rest = pl.ds(2 * i, 2), pl.ds(2 - 2 * i, 2)
            opposite, next_b = (b + 2) % SIDE, (b + k) % SIDE
            out.append(
                remote(
                    terms.at[u, opposite, half],
                    transit.at[u, i],
                    rs_send.at[u, i],
                    rs_recv.at[u, i],
                    along_b(par, k),
                )
            )
            out.append(
                remote(
                    terms.at[u, next_b, rest],
                    from_b.at[u, i, rest],
                    rs_send.at[u, 2 + i],
                    rs_recv.at[u, 2 + i],
                    along_b(par, k),
                )
            )
        return out

    def reduce_2(u, par):
        a, b = own_ab(par)
        out = []
        for i, k in enumerate((1, SIDE - 1)):
            half = pl.ds(2 * i, 2)
            out.append(
                remote(
                    transit.at[u, i],
                    from_b.at[u, i, half],
                    rs_send.at[u, 4 + i],
                    rs_recv.at[u, 4 + i],
                    along_b(par, k),
                )
            )
        return out

    def reduce_3(u, par):
        a, b = own_ab(par)
        return [
            remote(
                part.at[u, (a + k) % SIDE],
                from_a.at[u, k - 1],
                rs_send.at[u, 5 + k],
                rs_recv.at[u, 5 + k],
                along_a(par, k),
            )
            for k in range(1, SIDE)
        ]

    def ret_copy(u, i):
        j = u * PER_UNIT + i
        source = ep_plus(chips - j // 2, j % 2)
        return remote(
            result.at[u, pl.ds(i * cap, cap), :],
            ret_ref.at[ep],
            ret_send.at[j],
            ret_recv.at[j],
            {"ep": source},
        )

    def ret_in(j):
        return remote(
            result.at[0, pl.ds(0, cap), :],
            ret_ref.at[ep_plus(j // 2, j % 2)],
            ret_send.at[j],
            ret_recv.at[j],
            {"ep": ep_plus(j // 2, j % 2)},
        )

    def z_in(j):
        u, i = j // PER_UNIT, j % PER_UNIT
        a, b = own_ab(u % 2)
        return remote(
            out_ref.at[0],
            rows.at[u, b, a, pl.ds(i * cap, cap), :],
            z_send.at[j],
            z_recv.at[j],
            {"ep": ep_plus(chips - j // 2, j % 2)},
        )

    def stage_a0(u):
        par = u % 2
        for i in range(PER_UNIT):
            if i == 0:

                @pl.when(u > 0)
                def _():
                    z_in(u * PER_UNIT).wait_recv()

            else:
                z_in(u * PER_UNIT + i).wait_recv()
        start(gather_a(rows, u, par, *rows_sems))

    def stage_a1(u):
        par = u % 2
        arrive(gather_a_in(rows, u, par, *rows_sems))
        start(gather_b(rows, u, par, *rows_sems, back=False))

    def stage_a2(u):
        par = u % 2
        arrive(gather_b(rows, u, par, *rows_sems, back=True))
        start(gather_c(rows, u, par, *rows_sems, back=False))

    def stage_c(u):
        par = u % 2
        arrive(gather_c(rows, u, par, *rows_sems, back=True))

        @pl.when(u == 0)
        def _():
            for load in loads:
                load.wait()

        def at(t):
            y, x = t // SIDE, t % SIDE
            return y * (1 - par) + x * par, x * (1 - par) + y * par

        blocks = [rows[(u, *at(t))] for t in range(SIDE * SIDE)]
        x = jnp.concatenate(blocks, axis=1)
        gate = jnp.dot(x, wg[...], preferred_element_type=F32)
        up = jnp.dot(x, wu[...], preferred_element_type=F32)
        hidden = (gate / (1.0 + jnp.exp(-gate)) * up).astype(BF16)
        for t in range(SIDE * SIDE):
            term = jnp.dot(
                hidden, wd[:, t * LANES : (t + 1) * LANES], preferred_element_type=F32
            )
            terms[(u, *at(t))] = term.astype(BF16)
        start(reduce_1(u, par, False))

    def stage_r1(u):
        par = u % 2
        a, b = own_ab(par)
        for i, k in enumerate((1, SIDE - 1)):
            half = pl.ds(2 * i, 2)
            reduce_1(u, par, True)[2 * i].wait_recv()
            transit[u, i] = (
                transit[u, i].astype(F32) + terms[u, (b + k) % SIDE, half].astype(F32)
            ).astype(BF16)
            reduce_2(u, par)[i].start()

    def stage_r2(u):
        par = u % 2
        a, b = own_ab(par)
        first = reduce_1(u, par, True)
        arrive([first[1], first[3]])
        arrive(reduce_2(u, par))
        part[u] = (
            terms[u, b].astype(F32) + from_b[u, 0].astype(F32) + from_b[u, 1].astype(F32)
        ).astype(BF16)
        start(reduce_3(u, par))

    def stage_r3(u):
        par = u % 2
        a, b = own_ab(par)
        arrive(reduce_3(u, par))
        total = part[u, a].astype(F32)
        for k in range(SIDE - 1):
            total = total + from_a[u, k].astype(F32)
        result[u] = total.astype(BF16)
        for i in range(PER_UNIT):
            if i == 0:

                @pl.when(u == 0)
                def _():
                    ret_ref[ep] = result[0, 0:cap, :]

                @pl.when(u > 0)
                def _():
                    ret_copy(u, 0).start()

            else:
                ret_copy(u, i).start()

    stages = (
        (6, stage_r3),
        (5, stage_r2),
        (4, stage_r1),
        (2, stage_a2),
        (1, stage_a1),
        (0, stage_a0),
        (3, stage_c),
    )

    def step(s, carry):
        @pl.when(s == 1)
        def _():
            for h in range(2):
                arrive(gather_a_in(atts_ref, h, h, *att_sems))
                start(gather_b(atts_ref, h, h, *att_sems, back=False))

        @pl.when(s == 3)
        def _():
            for h in range(2):
                arrive(gather_b(atts_ref, h, h, *att_sems, back=True))
                start(gather_c(atts_ref, h, h, *att_sems, back=False))

        for lag, stage in stages:

            @pl.when((s >= lag) & (s < units + lag))
            def _(lag=lag, stage=stage):
                stage(s - lag)

        return carry

    lax.fori_loop(0, units + 6, step, 0)

    for h in range(2):
        arrive(gather_c(atts_ref, h, h, *att_sems, back=True))
        sent(gather_a(atts_ref, h, h, *att_sems))
        sent(gather_b(atts_ref, h, h, *att_sems, back=False))
        sent(gather_c(atts_ref, h, h, *att_sems, back=False))

    def drain(u, carry):
        par = u % 2
        sent(gather_a(rows, u, par, *rows_sems))
        sent(gather_b(rows, u, par, *rows_sems, back=False))
        sent(gather_c(rows, u, par, *rows_sems, back=False))
        sent(reduce_1(u, par, False))
        sent(reduce_2(u, par))
        sent(reduce_3(u, par))
        return carry

    lax.fori_loop(0, units, drain, 0)

    def drain_z(j, carry):
        z_copy(j).wait_send()
        ret_copy(j // PER_UNIT, j % PER_UNIT).wait_send()
        ret_in(j).wait_recv()
        return carry

    lax.fori_loop(1, senders, drain_z, 0)


def exchange(outgoing, attended, gate_weight, up_weight, down_weight):
    senders, cap, lanes = outgoing.shape
    units = senders // PER_UNIT
    unit_rows = PER_UNIT * cap
    half = attended.shape[1]
    tokens = attended.shape[2]
    vmem = pl.BlockSpec(memory_space=pltpu.VMEM)
    hbm = pl.BlockSpec(memory_space=pl.ANY)
    block = (unit_rows, lanes)
    dma = pltpu.SemaphoreType.DMA
    return pl.pallas_call(
        functools.partial(exchange_kernel, units),
        out_shape=(
            jax.ShapeDtypeStruct((senders, cap, lanes), BF16),
            jax.ShapeDtypeStruct((2, SIDE, SIDE, half, tokens), BF16),
        ),
        in_specs=[vmem, vmem, hbm, hbm, hbm],
        out_specs=(vmem, vmem),
        scratch_shapes=[
            pltpu.VMEM((units, SIDE, SIDE, *block), BF16),
            pltpu.VMEM((units, SIDE, SIDE, *block), BF16),
            pltpu.VMEM((units, 2, 2, *block), BF16),
            pltpu.VMEM((units, 2, SIDE, *block), BF16),
            pltpu.VMEM((units, SIDE, *block), BF16),
            pltpu.VMEM((units, SIDE - 1, *block), BF16),
            pltpu.VMEM((units, *block), BF16),
            pltpu.VMEM(gate_weight.shape, BF16),
            pltpu.VMEM(up_weight.shape, BF16),
            pltpu.VMEM(down_weight.shape, BF16),
            dma((3,)),
            dma((senders,)),
            dma((senders,)),
            dma((senders,)),
            dma((senders,)),
            dma((units, 7)),
            dma((units, 7)),
            dma((units, 9)),
            dma((units, 9)),
            dma((2, 7)),
            dma((2, 7)),
        ],
        compiler_params=pltpu.CompilerParams(
            collective_id=0, has_side_effects=True, vmem_limit_bytes=56 * 1024 * 1024
        ),
    )(outgoing, attended, gate_weight, up_weight, down_weight)


def local(
    query_proj,
    key_proj,
    value_proj,
    sink_logit,
    out_weight,
    expert_input,
    norm_gain,
    routes,
    route_weights,
    gate_weight,
    up_weight,
    down_weight,
):
    row_count, width = expert_input.shape
    expert_count = gate_weight.shape[0] * lax.axis_size("ep")
    cap = row_count * GROUPS // expert_count
    col_count = width // lax.axis_size(TP)

    widened = expert_input.astype(F32)
    scale = lax.rsqrt(jnp.mean(widened * widened, axis=1, keepdims=True) + NORM_EPS)
    first_col = lax.axis_index(TP) * col_count
    own_cols = lax.dynamic_slice_in_dim(expert_input, first_col, col_count, 1).astype(F32)
    own_gain = lax.dynamic_slice_in_dim(norm_gain, first_col, col_count, 0)
    normed = (own_cols * scale * own_gain).astype(BF16)

    experts = jnp.arange(expert_count, dtype=jnp.int32)
    hot = [(routes[:, k, None] == experts[None, :]) for k in range(2)]
    named = (hot[0] | hot[1]).astype(BF16)
    tokens = jnp.arange(row_count, dtype=jnp.int32)
    earlier = (tokens[None, :] < tokens[:, None]).astype(BF16)
    before = jnp.dot(earlier, named, preferred_element_type=F32)
    slots = [
        routes[:, k] * cap + jnp.sum(jnp.where(hot[k], before, 0.0), axis=1).astype(jnp.int32)
        for k in range(2)
    ]
    slot_ids = jnp.arange(expert_count * cap, dtype=jnp.int32)
    picks = [(slots[k][:, None] == slot_ids[None, :]) for k in range(2)]
    placed = (picks[0] | picks[1]).astype(BF16)
    outgoing = jnp.einsum("rs,rc->sc", placed, normed, preferred_element_type=F32)
    outgoing = outgoing.astype(BF16).reshape(expert_count, cap, col_count)

    attended = attend(query_proj, key_proj, value_proj, sink_logit)
    halves = attended.reshape(2, HEAD_DIM // 2, attended.shape[1])

    returned, gathered = exchange(outgoing, halves, gate_weight[0], up_weight[0], down_weight[0])

    by_head = out_weight.reshape(SIDE, SIDE, 2, HEAD_DIM // 2, out_weight.shape[1])
    first = by_head[:, :, 0]
    second = jnp.swapaxes(by_head[:, :, 1], 0, 1)
    weight = jnp.stack([first, second]).reshape(-1, out_weight.shape[1])
    flat = gathered.reshape(-1, gathered.shape[-1])
    mixer_out = jnp.einsum("fq,fd->qd", flat, weight, preferred_element_type=F32)

    returned = returned.reshape(expert_count * cap, col_count)
    combined = 0.0
    for k in range(2):
        picked = jnp.dot(picks[k].astype(BF16), returned, preferred_element_type=F32)
        combined = combined + picked * route_weights[:, k, None]
    return (mixer_out.astype(BF16), combined.astype(BF16))


def solution(mesh):
    finer = Mesh(mesh.devices.reshape(mesh.shape["ep"], SIDE, SIDE), ("ep", "tp_0", "tp_1"))
    in_specs = (
        P("ep", TP),
        P("ep", None),
        P("ep", None),
        P(TP),
        P(None, TP),
        P("ep", None),
        P(),
        P("ep", None),
        P("ep", None),
        P("ep", None, TP),
        P("ep", None, TP),
        P("ep", TP, None),
    )
    out_specs = (P("ep", TP), P("ep", TP))
    return jax.shard_map(local, mesh=finer, in_specs=in_specs, out_specs=out_specs, check_vma=False)
```

```python
import functools

import jax
import jax.numpy as jnp
from jax import lax
from jax.experimental import pallas as pl
from jax.experimental.pallas import tpu as pltpu
from jax.sharding import Mesh
from jax.sharding import PartitionSpec as P

HEADS = 16
KV_HEADS = 4
HEAD_DIM = 64
HALF_WIN = 128
GROUPS = 4
TOP_K = 2
NORM_EPS = 1e-06
ROPE_BASE = 10000.0
NEG_BIG = -1e30
TP = ("tp_0", "tp_1")
SIDE = 4
LANES = 128
PER_UNIT = 4
BF16 = jnp.bfloat16
F32 = jnp.float32
MESH = pl.DeviceIdType.MESH

Z_ORDER = (0, 1, 2, 3, 9, 4, 10, 11, 12, 5, 6, 7, 13, 8, 14, 15)
Z_ARRIVAL = (0, 2.5, 4, 5.8, 8, 10.5, 13.3, 16.5, 20, 9.2, 10.5, 11.5, 12, 12.4, 12.4, 12)
RELAY = {0: 1, 1: 1, 3: -1, 2: -1}


def plan(units):
    piece, rate, latency = 32.0, 45.56, 2.4
    cost = {"Q": 0.6, "A0": 0.08, "A1": 0.05, "A2": 0.04, "C": 1.0, "P": 0.5}
    cost.update({"R1": 0.15, "R2": 0.3, "R3": 0.25})
    stage = ("Q", "A0", "A1", "A2", "C", "P", "R1", "R2", "R3")
    free, arrival, pending = {}, {}, {}

    def send(now, lanes, size, token, extra=0.0):
        ends = []
        for lane in lanes:
            free[lane] = max(free.get(lane, 0.0), now) + size / rate
            ends.append(free[lane])
        arrival[token] = max(ends) + latency + extra

    per = PER_UNIT // 2
    for u in range(units):
        arrival[("z", u)] = max(Z_ARRIVAL[k] for k in Z_ORDER[u * per : u * per + per])
    for i, ready in enumerate((3.5, 0.0, 0.0, 3.5)):
        arrival[("q", i)] = ready
        pending[("Q", i)] = [("q", i)]
    for u in range(units + 2):
        att = u - units
        first = [("z", u)] if att < 0 else [("Q", 2 * att), ("Q", 2 * att + 1)]
        pending[("A0", u)] = first
        for k in (1, 3, 2):
            pending[("A1", u, k)] = [("a", u, k)]
        for k, s in RELAY.items():
            pending[("A2", u, k)] = [("b", u, k, s)]
        rest = [("b", u, k, s) for k in range(SIDE) for s in (1, -1)]
        rest += [("c", u, k) for k in range(SIDE)]
        pending[("C" if att < 0 else "P", u)] = rest
        if att < 0:
            for i in range(2):
                pending[("R1", u, i)] = [("t", u, i)]
            pending[("R2", u)] = [("f", u, i, j) for i in range(2) for j in range(2)]
            pending[("R3", u)] = [("g", u, k) for k in (1, 2, 3)]

    now, order = 0.0, []
    while pending:
        ready, later = [], []
        for event, needs in pending.items():
            if all(need in arrival for need in needs):
                at = max(arrival[need] for need in needs)
                if at <= now:
                    kind, u = event[0], event[1]
                    place = -1 if kind == "Q" or u >= units else u
                    late = stage.index(kind) >= 4
                    ready.append((late, place, -stage.index(kind), event))
                else:
                    later.append(at)
        if not ready:
            now = min(later)
            continue
        event = min(ready)[-1]
        del pending[event]
        order.append(event)
        kind, u = event[:2]
        now += cost[kind]
        a, b = ("x", "y") if u % 2 == 0 else ("y", "x")
        both = ((a, 1), (a, -1))
        if kind == "Q":
            arrival[event] = now
        elif kind == "A0":
            send(now, both[:1], piece, ("a", u, 1))
            send(now, both[1:], piece, ("a", u, 3))
            send(now, both, piece, ("a", u, 2), 0.7)
        if kind in ("A0", "A1"):
            k = 0 if kind == "A0" else event[2]
            for s in (1, -1):
                send(now, ((b, s),), piece, ("b", u, k, s))
        elif kind == "A2":
            send(now, ((b, RELAY[event[2]]),), piece, ("c", u, event[2]))
        elif kind == "C":
            for i, s in enumerate((1, -1)):
                send(now, ((b, s),), 2 * piece, ("t", u, i))
            for i, s in enumerate((1, -1)):
                send(now, ((b, s),), 2 * piece, ("f", u, i, 0))
        elif kind == "R1":
            send(now, ((b, 1 - 2 * event[2]),), 2 * piece, ("f", u, event[2], 1))
        elif kind == "R2":
            send(now, both[:1], piece, ("g", u, 1))
            send(now, both[1:], piece, ("g", u, 3))
            send(now, both, piece, ("g", u, 2), 0.7)
    return order


def layer_kernel(
    units,
    order,
    query_ref,
    key_ref,
    value_ref,
    freq_ref,
    sink_ref,
    input_ref,
    gain_ref,
    routes_ref,
    weights_ref,
    wo_hbm,
    wg_hbm,
    wu_hbm,
    wd_hbm,
    mixer_ref,
    expert_ref,
    out,
    picks,
    ext,
    rot_q,
    att,
    returned,
    rows,
    terms,
    transit,
    from_b,
    part,
    from_a,
    result,
    wo,
    wg,
    wu,
    wd,
    w_sem,
    halo_send,
    halo_recv,
    z_send,
    z_recv,
    ret_send,
    ret_recv,
    ag_send,
    ag_recv,
    rs_send,
    rs_recv,
):
    ep = lax.axis_index("ep")
    yi = lax.axis_index("tp_0")
    xi = lax.axis_index("tp_1")
    tp = yi * SIDE + xi
    senders = units * PER_UNIT
    chips = senders // 2
    zi = ep // 2
    ci = ep % 2
    cap = out.shape[1]
    tokens = query_ref.shape[0]
    blocks = tokens // HALF_WIN

    def distance(j):
        return Z_ORDER[j // 2]

    def ep_plus(step, flip):
        return ((zi + step) % chips) * 2 + (ci + flip) % 2

    def along_a(par, k):
        return {"tp_0": (yi + k * par) % SIDE, "tp_1": (xi + k * (1 - par)) % SIDE}

    def along_b(par, k):
        return along_a(1 - par, k)

    def own_ab(par):
        return (xi, yi) if par == 0 else (yi, xi)

    def remote(src, dst, ssem, rsem, dev):
        return pltpu.make_async_remote_copy(
            src_ref=src,
            dst_ref=dst,
            send_sem=ssem,
            recv_sem=rsem,
            device_id=dev,
            device_id_type=MESH,
        )

    to_load = ((wg_hbm, wg), (wu_hbm, wu), (wd_hbm, wd), (wo_hbm, wo))
    loads = [pltpu.make_async_copy(s, d, w_sem.at[i]) for i, (s, d) in enumerate(to_load)]
    for load in loads:
        load.start()

    barrier = pltpu.get_barrier_semaphore()
    for j in range(1, senders):
        pl.semaphore_signal(
            barrier, inc=1, device_id={"ep": ep_plus(j // 2, j % 2)}, device_id_type=MESH
        )
    for par in range(2):
        for k in range(1, SIDE):
            pl.semaphore_signal(barrier, inc=1, device_id=along_a(par, k), device_id_type=MESH)

    row_count, width = input_ref.shape
    widened = input_ref[...].astype(F32)
    scale = lax.rsqrt(jnp.mean(widened * widened, axis=1, keepdims=True) + NORM_EPS)
    cols = pl.ds(pl.multiple_of(tp * LANES, LANES), LANES)
    normed = (input_ref[:, cols].astype(F32) * scale * gain_ref[:, cols]).astype(BF16)
    routes = routes_ref[...]
    lane = lax.broadcasted_iota(jnp.int32, (row_count, LANES), 1)
    hot = [routes[:, k : k + 1] == lane for k in range(TOP_K)]
    named = jnp.where(hot[0] | hot[1], 1.0, 0.0).astype(BF16)
    square = (row_count, row_count)
    down, across = (lax.broadcasted_iota(jnp.int32, square, d) for d in range(2))
    earlier = jnp.where(across < down, 1.0, 0.0).astype(BF16)
    before = jnp.dot(earlier, named, preferred_element_type=F32)
    slot_ids = lax.broadcasted_iota(jnp.int32, (row_count, senders * cap), 1)
    for k in range(TOP_K):
        rank = jnp.sum(jnp.where(hot[k], before, 0.0), axis=1, keepdims=True)
        slot = routes[:, k : k + 1] * cap + rank.astype(jnp.int32)
        picks[k] = jnp.where(slot == slot_ids, 1.0, 0.0).astype(BF16)
    placed = picks[0] + picks[1]
    outgoing = lax.dot_general(
        placed, normed, (((0,), (0,)), ((), ())), preferred_element_type=F32
    )
    out[...] = outgoing.astype(BF16).reshape(senders, cap, LANES)

    first_row = ep * tokens
    position = lax.broadcasted_iota(jnp.int32, (tokens, LANES), 0) + first_row
    angles = position.astype(F32) * freq_ref[...]
    cosine, sine = jnp.cos(angles), jnp.sin(angles)

    def selector(depth, first, target, turned):
        shape = (depth, LANES)
        r, c = (lax.broadcasted_iota(jnp.int32, shape, d) for d in range(2))
        inside = (c >= target) & (c < target + HEAD_DIM)
        at = first + c - target
        if not turned:
            return jnp.where(inside & (r == at), 1.0, 0.0).astype(BF16)
        low = c < HEAD_DIM // 2
        half = HEAD_DIM // 2
        sign = jnp.where(low & (r == at + half), -1.0, 0.0)
        sign = sign + jnp.where(~low & (r == at - half), 1.0, 0.0)
        return jnp.where(inside, sign, 0.0).astype(BF16)

    def dot(a, b):
        return jnp.dot(a, b, preferred_element_type=F32)

    depth = key_ref.shape[1]
    own = (tp // (HEADS // KV_HEADS)) * HEAD_DIM
    keys = key_ref[...]
    plain = dot(keys, selector(depth, own, 0, False))
    plain = plain + dot(value_ref[...], selector(depth, own, HEAD_DIM, False))
    turned = dot(keys, selector(depth, own, 0, True))
    ext[HALF_WIN : HALF_WIN + tokens] = (plain * cosine + turned * sine).astype(BF16)
    query = query_ref[...]
    plain = dot(query, selector(HEAD_DIM, 0, 0, False))
    turned = dot(query, selector(HEAD_DIM, 0, 0, True))
    rot_q[...] = (plain * cosine + turned * sine).astype(BF16)

    pl.semaphore_wait(barrier, senders - 1 + 2 * (SIDE - 1))

    def z_copy(j):
        u, i = j // PER_UNIT, j % PER_UNIT
        a, b = own_ab(u % 2)
        dest = ep_plus(distance(j), j % 2)
        return remote(
            out.at[dest],
            rows.at[u, b, a, pl.ds(i * cap, cap), :],
            z_send.at[j],
            z_recv.at[j],
            {"ep": dest},
        )

    def halo_copy(i):
        source = tokens if i == 0 else HALF_WIN
        target = 0 if i == 0 else HALF_WIN + tokens
        return remote(
            ext.at[pl.ds(source, HALF_WIN)],
            ext.at[pl.ds(target, HALF_WIN)],
            halo_send.at[i],
            halo_recv.at[i],
            {"ep": (ep + (1 if i == 0 else senders - 1)) % senders},
        )

    for j in range(1, 4):
        z_copy(j).start()
    for i in range(2):
        halo_copy(i).start()
    for j in range(4, senders):
        z_copy(j).start()
    a0, b0 = own_ab(0)
    rows[0, b0, a0, 0:cap, :] = out[ep]

    def attend(i):
        if i == 0:
            halo_copy(0).wait_recv()
        if i == blocks - 1:
            halo_copy(1).wait_recv()
        near = 3 * HALF_WIN
        window = ext[i * HALF_WIN : i * HALF_WIN + near]
        block_q = rot_q[i * HALF_WIN : (i + 1) * HALF_WIN]
        scores = lax.dot_general(
            block_q, window, (((1,), (1,)), ((), ())), preferred_element_type=F32
        ) * HEAD_DIM ** (-0.5)
        shape = (HALF_WIN, near)
        q_at, k_at = (lax.broadcasted_iota(jnp.int32, shape, d) for d in range(2))
        gap = k_at - q_at
        global_key = first_row + (i - 1) * HALF_WIN + k_at
        allowed = (gap >= 0) & (gap <= 2 * HALF_WIN)
        allowed = allowed & (global_key >= 0) & (global_key < senders * tokens)
        scores = jnp.where(allowed, scores, NEG_BIG)
        sink = sink_ref[...]
        row_peak = jnp.maximum(jnp.max(scores, axis=1, keepdims=True), sink)
        lifted = jnp.exp(scores - row_peak)
        norm_total = jnp.sum(lifted, axis=1, keepdims=True) + jnp.exp(sink - row_peak)
        probs = (lifted / norm_total).astype(BF16)
        weighted = dot(probs, window)
        a, b = own_ab((i // 2) % 2)
        piece_cols = slice((i % 2) * HALF_WIN, (i % 2 + 1) * HALF_WIN)
        att[i // 2, b, a, :, piece_cols] = weighted.T[HEAD_DIM:].astype(BF16)

    def buffer(u):
        return (rows, u) if u < units else (att, u - units)

    def gather_a(u, k, back=False):
        par = u % 2
        a, b = own_ab(par)
        buf, at = buffer(u)
        return remote(
            buf.at[at, b, a],
            buf.at[at, b, (a + SIDE - k) % SIDE if back else a],
            ag_send.at[u, k - 1],
            ag_recv.at[u, k - 1],
            along_a(par, k),
        )

    def gather_b(u, k, s, back=False):
        par = u % 2
        a, b = own_ab(par)
        buf, at = buffer(u)
        col = (a + SIDE - k) % SIDE
        sem = 3 + 2 * k + (0 if s == 1 else 1)
        return remote(
            buf.at[at, b, col],
            buf.at[at, (b + SIDE - s) % SIDE if back else b, col],
            ag_send.at[u, sem],
            ag_recv.at[u, sem],
            along_b(par, s % SIDE),
        )

    def gather_c(u, k, back=False):
        par = u % 2
        a, b = own_ab(par)
        buf, at = buffer(u)
        s = RELAY[k]
        col = (a + SIDE - k) % SIDE
        held = (b + SIDE - s) % SIDE
        return remote(
            buf.at[at, held, col],
            buf.at[at, (b + 2) % SIDE if back else held, col],
            ag_send.at[u, 11 + k],
            ag_recv.at[u, 11 + k],
            along_b(par, s % SIDE),
        )

    turns = ((0, 1), (1, SIDE - 1))

    def reduce_opposite(u, i, k):
        par = u % 2
        a, b = own_ab(par)
        return remote(
            terms.at[u, (b + 2) % SIDE, pl.ds(2 * i, 2)],
            transit.at[u, i],
            rs_send.at[u, i],
            rs_recv.at[u, i],
            along_b(par, k),
        )

    def reduce_next(u, i, k):
        par = u % 2
        a, b = own_ab(par)
        rest = pl.ds(2 - 2 * i, 2)
        return remote(
            terms.at[u, (b + k) % SIDE, rest],
            from_b.at[u, i, rest],
            rs_send.at[u, 2 + i],
            rs_recv.at[u, 2 + i],
            along_b(par, k),
        )

    def reduce_relay(u, i, k):
        return remote(
            transit.at[u, i],
            from_b.at[u, i, pl.ds(2 * i, 2)],
            rs_send.at[u, 4 + i],
            rs_recv.at[u, 4 + i],
            along_b(u % 2, k),
        )

    def reduce_a(u, k):
        a, b = own_ab(u % 2)
        return remote(
            part.at[u, (a + k) % SIDE],
            from_a.at[u, k - 1],
            rs_send.at[u, 5 + k],
            rs_recv.at[u, 5 + k],
            along_a(u % 2, k),
        )

    def ret_copy(j):
        source = ep_plus(chips - distance(j), j % 2)
        return remote(
            result.at[j // PER_UNIT, pl.ds((j % PER_UNIT) * cap, cap), :],
            returned.at[ep],
            ret_send.at[j],
            ret_recv.at[j],
            {"ep": source},
        )

    def gathered(u):
        for k, s in RELAY.items():
            gather_b(u, k, -s, back=True).wait_recv()
            gather_c(u, k, back=True).wait_recv()
        buf, at = buffer(u)
        if u % 2 == 0:
            places = [(t // SIDE, t % SIDE) for t in range(SIDE * SIDE)]
        else:
            places = [(t % SIDE, t // SIDE) for t in range(SIDE * SIDE)]
        return places, [buf[(at, *place)] for place in places]

    loaded = []

    def expert(u):
        places, pieces = gathered(u)
        if not loaded:
            loaded.append(u)
            for load in loads[:3]:
                load.wait()
        x = jnp.concatenate(pieces, axis=1)
        gate = dot(x, wg[...])
        up = dot(x, wu[...])
        hidden = (gate / (1.0 + jnp.exp(-gate)) * up).astype(BF16)
        for t, place in enumerate(places):
            terms[(u, *place)] = dot(hidden, wd[:, t * LANES : (t + 1) * LANES]).astype(BF16)
        for i, k in turns:
            reduce_opposite(u, i, k).start()
        for i, k in turns:
            reduce_next(u, i, k).start()

    projected = []

    def project(u):
        places, pieces = gathered(u)
        if not projected:
            loads[3].wait()
        projected.append(u)
        x = jnp.concatenate(pieces, axis=0)
        half = x.shape[1]
        at = (u - units) * half
        total = lax.dot_general(x, wo[...], (((0,), (0,)), ((), ())), preferred_element_type=F32)
        mixer_ref[at : at + half] = total.astype(BF16)

    for event in order:
        kind, u = event[:2]
        a, b = own_ab(u % 2)
        if kind == "Q":
            attend(u)
        elif kind == "A0":
            if u < units:
                for j in range(u * PER_UNIT, (u + 1) * PER_UNIT):
                    if j:
                        z_copy(j).wait_recv()
            for k in (1, 3, 2):
                gather_a(u, k).start()
            for s in (1, -1):
                gather_b(u, 0, s).start()
        elif kind == "A1":
            k = event[2]
            gather_a(u, k, back=True).wait_recv()
            for s in (1, -1):
                gather_b(u, k, s).start()
        elif kind == "A2":
            k = event[2]
            gather_b(u, k, RELAY[k], back=True).wait_recv()
            gather_c(u, k).start()
        elif kind == "C":
            expert(u)
        elif kind == "P":
            project(u)
        elif kind == "R1":
            i, k = turns[event[2]]
            reduce_opposite(u, i, k).wait_recv()
            held = terms[u, (b + k) % SIDE, 2 * i : 2 * i + 2]
            transit[u, i] = (transit[u, i].astype(F32) + held.astype(F32)).astype(BF16)
            reduce_relay(u, i, k).start()
        elif kind == "R2":
            for i, k in turns:
                reduce_next(u, i, k).wait_recv()
                reduce_relay(u, i, k).wait_recv()
            part[u] = (
                terms[u, b].astype(F32) + from_b[u, 0].astype(F32) + from_b[u, 1].astype(F32)
            ).astype(BF16)
            for k in (1, 3, 2):
                reduce_a(u, k).start()
        elif kind == "R3":
            total = part[u, a].astype(F32)
            for k in (1, 3, 2):
                reduce_a(u, k).wait_recv()
                total = total + from_a[u, k - 1].astype(F32)
            result[u] = total.astype(BF16)
            for j in range(u * PER_UNIT, (u + 1) * PER_UNIT):
                if j:
                    ret_copy(j).start()
                else:
                    returned[ep] = result[0, 0:cap, :]

    for u in range(units + 2):
        for k in (1, 3, 2):
            gather_a(u, k).wait_send()
        for k in range(SIDE):
            for s in (1, -1):
                gather_b(u, k, s).wait_send()
            gather_c(u, k).wait_send()
    for u in range(units):
        for i, k in turns:
            reduce_opposite(u, i, k).wait_send()
            reduce_next(u, i, k).wait_send()
            reduce_relay(u, i, k).wait_send()
        for k in (1, 3, 2):
            reduce_a(u, k).wait_send()
    for i in range(2):
        halo_copy(i).wait_send()
    for j in range(1, senders):
        z_copy(j).wait_send()
    for j in range(1, senders):
        ret_copy(j).wait()
    back = returned[...].reshape(senders * cap, LANES)
    combined = dot(picks[0], back) * weights_ref[:, 0:1]
    combined = combined + dot(picks[1], back) * weights_ref[:, 1:2]
    expert_ref[...] = combined.astype(BF16)


def local(
    query_proj,
    key_proj,
    value_proj,
    sink_logit,
    out_weight,
    expert_input,
    norm_gain,
    routes,
    route_weights,
    gate_weight,
    up_weight,
    down_weight,
):
    row_count, width = expert_input.shape
    tokens = query_proj.shape[0]
    senders = gate_weight.shape[0] * lax.axis_size("ep")
    cap = row_count * GROUPS // senders
    units = senders // PER_UNIT
    half_dim = HEAD_DIM // 2
    inverse_freq = 1.0 / ROPE_BASE ** (jnp.arange(half_dim, dtype=F32) * 2.0 / HEAD_DIM)
    zeros = jnp.zeros((LANES - HEAD_DIM,), F32)
    freq = jnp.concatenate([inverse_freq, inverse_freq, zeros])[None, :]

    vmem = pl.BlockSpec(memory_space=pltpu.VMEM)
    hbm = pl.BlockSpec(memory_space=pl.ANY)
    dma = pltpu.SemaphoreType.DMA
    block = (PER_UNIT * cap, LANES)
    gate, up, down = gate_weight[0], up_weight[0], down_weight[0]
    return pl.pallas_call(
        functools.partial(layer_kernel, units, plan(units)),
        out_shape=(
            jax.ShapeDtypeStruct((tokens, LANES), BF16),
            jax.ShapeDtypeStruct((row_count, LANES), BF16),
        ),
        in_specs=[vmem] * 9 + [hbm] * 4,
        out_specs=(vmem, vmem),
        scratch_shapes=[
            pltpu.VMEM((senders, cap, LANES), BF16),
            pltpu.VMEM((TOP_K, row_count, senders * cap), BF16),
            pltpu.VMEM((tokens + 2 * HALF_WIN, LANES), BF16),
            pltpu.VMEM((tokens, LANES), BF16),
            pltpu.VMEM((2, SIDE, SIDE, HEAD_DIM, tokens // 2), BF16),
            pltpu.VMEM((senders, cap, LANES), BF16),
            pltpu.VMEM((units, SIDE, SIDE, *block), BF16),
            pltpu.VMEM((units, SIDE, SIDE, *block), BF16),
            pltpu.VMEM((units, 2, 2, *block), BF16),
            pltpu.VMEM((units, 2, SIDE, *block), BF16),
            pltpu.VMEM((units, SIDE, *block), BF16),
            pltpu.VMEM((units, SIDE - 1, *block), BF16),
            pltpu.VMEM((units, *block), BF16),
            pltpu.VMEM(out_weight.shape, BF16),
            pltpu.VMEM(gate.shape, BF16),
            pltpu.VMEM(up.shape, BF16),
            pltpu.VMEM(down.shape, BF16),
            dma((4,)),
            dma((2,)),
            dma((2,)),
            dma((senders,)),
            dma((senders,)),
            dma((senders,)),
            dma((senders,)),
            dma((units + 2, 15)),
            dma((units + 2, 15)),
            dma((units, 9)),
            dma((units, 9)),
        ],
        compiler_params=pltpu.CompilerParams(
            collective_id=0, has_side_effects=True, vmem_limit_bytes=56 * 1024 * 1024
        ),
    )(
        query_proj,
        key_proj,
        value_proj,
        freq,
        sink_logit.reshape(1, 1),
        expert_input,
        norm_gain[None, :],
        routes,
        route_weights,
        out_weight,
        gate,
        up,
        down,
    )


def solution(mesh):
    finer = Mesh(mesh.devices.reshape(mesh.shape["ep"], SIDE, SIDE), ("ep", "tp_0", "tp_1"))
    in_specs = (
        P("ep", TP),
        P("ep", None),
        P("ep", None),
        P(TP),
        P(None, TP),
        P("ep", None),
        P(),
        P("ep", None),
        P("ep", None),
        P("ep", None, TP),
        P("ep", None, TP),
        P("ep", TP, None),
    )
    out_specs = (P("ep", TP), P("ep", TP))
    return jax.shard_map(local, mesh=finer, in_specs=in_specs, out_specs=out_specs, check_vma=False)
```

```python
import functools

import jax
import jax.numpy as jnp
import numpy as np
from jax import lax
from jax.experimental import pallas as pl
from jax.experimental.pallas import tpu as pltpu
from jax.sharding import Mesh
from jax.sharding import PartitionSpec as P

HEADS = 16
KV_HEADS = 4
HEAD_DIM = 64
HALF_WIN = 128
GROUPS = 4
TOP_K = 2
NORM_EPS = 1e-06
ROPE_BASE = 10000.0
NEG_BIG = -1e30
TP = ("tp_0", "tp_1")
SIDE = 4
LANES = 128
PER_UNIT = 4
BF16 = jnp.bfloat16
F32 = jnp.float32
MESH = pl.DeviceIdType.MESH

Z_ORDER = (0, 1, 2, 3, 9, 4, 10, 11, 12, 5, 6, 7, 13, 8, 14, 15)
Z_ARRIVAL = (0, 2.5, 4, 5.8, 8, 10.5, 13.3, 16.5, 20, 9.2, 10.5, 11.5, 12, 12.4, 12.4, 12)
RELAY = {0: 1, 1: 1, 3: -1, 2: -1}


def plan(units):
    piece, rate, latency = 32.0, 45.56, 2.4
    cost = {"Q": 0.6, "A0": 0.08, "A1": 0.05, "A2": 0.04, "C": 1.0, "P": 0.5}
    cost.update({"R1": 0.15, "R2": 0.3, "R3": 0.25})
    stage = ("Q", "A0", "A1", "A2", "C", "P", "R1", "R2", "R3")
    free, arrival, pending = {}, {}, {}

    def send(now, lanes, size, token, extra=0.0):
        ends = []
        for lane in lanes:
            free[lane] = max(free.get(lane, 0.0), now) + size / rate
            ends.append(free[lane])
        arrival[token] = max(ends) + latency + extra

    per = PER_UNIT // 2
    for u in range(units):
        arrival[("z", u)] = max(Z_ARRIVAL[k] for k in Z_ORDER[u * per : u * per + per])
    for i, ready in enumerate((3.5, 0.0, 0.0, 3.5)):
        arrival[("q", i)] = ready
        pending[("Q", i)] = [("q", i)]
    for u in range(units + 2):
        att = u - units
        first = [("z", u)] if att < 0 else [("Q", 2 * att), ("Q", 2 * att + 1)]
        pending[("A0", u)] = first
        for k in (1, 3, 2):
            pending[("A1", u, k)] = [("a", u, k)]
        for k, s in RELAY.items():
            pending[("A2", u, k)] = [("b", u, k, s)]
        rest = [("b", u, k, s) for k in range(SIDE) for s in (1, -1)]
        rest += [("c", u, k) for k in range(SIDE)]
        pending[("C" if att < 0 else "P", u)] = rest
        if att < 0:
            for i in range(2):
                pending[("R1", u, i)] = [("t", u, i)]
            pending[("R2", u)] = [("f", u, i, j) for i in range(2) for j in range(2)]
            pending[("R3", u)] = [("g", u, k) for k in (1, 2, 3)]

    now, order = 0.0, []
    while pending:
        ready, later = [], []
        for event, needs in pending.items():
            if all(need in arrival for need in needs):
                at = max(arrival[need] for need in needs)
                if at <= now:
                    kind, u = event[0], event[1]
                    place = -1 if kind == "Q" or u >= units else u
                    late = stage.index(kind) >= 4
                    ready.append((late, place, -stage.index(kind), event))
                else:
                    later.append(at)
        if not ready:
            now = min(later)
            continue
        event = min(ready)[-1]
        del pending[event]
        order.append(event)
        kind, u = event[:2]
        now += cost[kind]
        a, b = ("x", "y") if u % 2 == 0 else ("y", "x")
        both = ((a, 1), (a, -1))
        if kind == "Q":
            arrival[event] = now
        elif kind == "A0":
            send(now, both[:1], piece, ("a", u, 1))
            send(now, both[1:], piece, ("a", u, 3))
            send(now, both, piece, ("a", u, 2), 0.7)
        if kind in ("A0", "A1"):
            k = 0 if kind == "A0" else event[2]
            for s in (1, -1):
                send(now, ((b, s),), piece, ("b", u, k, s))
        elif kind == "A2":
            send(now, ((b, RELAY[event[2]]),), piece, ("c", u, event[2]))
        elif kind == "C":
            for i, s in enumerate((1, -1)):
                send(now, ((b, s),), 2 * piece, ("t", u, i))
            for i, s in enumerate((1, -1)):
                send(now, ((b, s),), 2 * piece, ("f", u, i, 0))
        elif kind == "R1":
            send(now, ((b, 1 - 2 * event[2]),), 2 * piece, ("f", u, event[2], 1))
        elif kind == "R2":
            send(now, both[:1], piece, ("g", u, 1))
            send(now, both[1:], piece, ("g", u, 3))
            send(now, both, piece, ("g", u, 2), 0.7)
    return order


def layer_kernel(
    units,
    order,
    sink_ref,
    input_hbm,
    gain_hbm,
    routes_hbm,
    key_hbm,
    value_hbm,
    query_hbm,
    freq_hbm,
    weights_hbm,
    wg_hbm,
    wu_hbm,
    wd_hbm,
    wo_hbm,
    mixer_ref,
    expert_ref,
    out,
    picks,
    raw,
    ext,
    rot_q,
    att,
    returned,
    rows,
    terms,
    transit,
    from_b,
    part,
    from_a,
    result,
    input_ref,
    gain_ref,
    routes_ref,
    key_ref,
    value_ref,
    query_ref,
    freq_ref,
    weights_ref,
    wg,
    wu,
    wd,
    wo,
    load_sem,
    halo_send,
    halo_recv,
    z_send,
    z_recv,
    ret_send,
    ret_recv,
    ag_send,
    ag_recv,
    rs_send,
    rs_recv,
):
    ep = lax.axis_index("ep")
    yi = lax.axis_index("tp_0")
    xi = lax.axis_index("tp_1")
    tp = yi * SIDE + xi
    senders = units * PER_UNIT
    chips = senders // 2
    zi = ep // 2
    ci = ep % 2
    cap = out.shape[1]
    tokens = query_ref.shape[1]
    blocks = tokens // HALF_WIN

    def distance(j):
        return Z_ORDER[j // 2]

    def ep_plus(step, flip):
        return ((zi + step) % chips) * 2 + (ci + flip) % 2

    def along_a(par, k):
        return {"tp_0": (yi + k * par) % SIDE, "tp_1": (xi + k * (1 - par)) % SIDE}

    def along_b(par, k):
        return along_a(1 - par, k)

    def own_ab(par):
        return (xi, yi) if par == 0 else (yi, xi)

    def remote(src, dst, ssem, rsem, dev):
        return pltpu.make_async_remote_copy(
            src_ref=src,
            dst_ref=dst,
            send_sem=ssem,
            recv_sem=rsem,
            device_id=dev,
            device_id_type=MESH,
        )

    barrier = pltpu.get_barrier_semaphore()
    for j in range(1, senders):
        pl.semaphore_signal(
            barrier, inc=1, device_id={"ep": ep_plus(j // 2, j % 2)}, device_id_type=MESH
        )
    for par in range(2):
        for k in range(1, SIDE):
            pl.semaphore_signal(barrier, inc=1, device_id=along_a(par, k), device_id_type=MESH)

    to_load = (
        (input_hbm, input_ref),
        (gain_hbm, gain_ref),
        (routes_hbm, routes_ref),
        (key_hbm, key_ref),
        (value_hbm, value_ref),
        (query_hbm, query_ref),
        (freq_hbm, freq_ref),
        (weights_hbm, weights_ref),
        (wg_hbm, wg),
        (wu_hbm, wu),
        (wd_hbm, wd),
        (wo_hbm, wo),
    )
    loads = [pltpu.make_async_copy(s, d, load_sem.at[i]) for i, (s, d) in enumerate(to_load)]
    for load in loads:
        load.start()

    def upright(row):
        return jnp.broadcast_to(row, (LANES, row.shape[1])).T

    row_count = input_ref.shape[0]
    for load in loads[:3]:
        load.wait()
    widened = input_ref[...].astype(F32)
    scale = lax.rsqrt(jnp.mean(widened * widened, axis=1, keepdims=True) + NORM_EPS)
    cols = pl.ds(pl.multiple_of(tp * LANES, LANES), LANES)
    normed = (input_ref[:, cols].astype(F32) * scale * gain_ref[:, cols]).astype(BF16)
    routes = routes_ref[...].astype(F32)
    named_by = [upright(routes[k : k + 1]) for k in range(TOP_K)]
    lane = lax.broadcasted_iota(jnp.int32, (row_count, LANES), 1).astype(F32)
    hot = [named_by[k] == lane for k in range(TOP_K)]
    named = jnp.where(hot[0] | hot[1], 1.0, 0.0).astype(BF16)
    square = (row_count, row_count)
    down, across = (lax.broadcasted_iota(jnp.int32, square, d) for d in range(2))
    earlier = jnp.where(across < down, 1.0, 0.0).astype(BF16)
    before = jnp.dot(earlier, named, preferred_element_type=F32)
    slot_ids = lax.broadcasted_iota(jnp.int32, (row_count, senders * cap), 1)
    for k in range(TOP_K):
        rank = jnp.sum(jnp.where(hot[k], before, 0.0), axis=1, keepdims=True)
        slot = (named_by[k][:, 0:1] * cap + rank).astype(jnp.int32)
        picks[k] = jnp.where(slot == slot_ids, 1.0, 0.0).astype(BF16)
    placed = picks[0] + picks[1]
    outgoing = lax.dot_general(
        placed, normed, (((0,), (0,)), ((), ())), preferred_element_type=F32
    )
    out[...] = outgoing.astype(BF16).reshape(senders, cap, LANES)

    first_row = ep * tokens

    def selector(depth, first, target, turned):
        shape = (depth, LANES)
        r, c = (lax.broadcasted_iota(jnp.int32, shape, d) for d in range(2))
        inside = (c >= target) & (c < target + HEAD_DIM)
        at = first + c - target
        if not turned:
            return jnp.where(inside & (r == at), 1.0, 0.0).astype(BF16)
        low = c < HEAD_DIM // 2
        half = HEAD_DIM // 2
        sign = jnp.where(low & (r == at + half), -1.0, 0.0)
        sign = sign + jnp.where(~low & (r == at - half), 1.0, 0.0)
        return jnp.where(inside, sign, 0.0).astype(BF16)

    def dot(a, b):
        return jnp.dot(a, b, preferred_element_type=F32)

    for load in loads[3:5]:
        load.wait()
    depth = key_ref.shape[1]
    own = (tp // (HEADS // KV_HEADS)) * HEAD_DIM
    plain = dot(key_ref[...], selector(depth, own, 0, False))
    plain = plain + dot(value_ref[...], selector(depth, own, HEAD_DIM, False))
    raw[HALF_WIN : HALF_WIN + tokens] = plain.astype(BF16)

    pl.semaphore_wait(barrier, senders - 1 + 2 * (SIDE - 1))

    def z_copy(j):
        u, i = j // PER_UNIT, j % PER_UNIT
        a, b = own_ab(u % 2)
        dest = ep_plus(distance(j), j % 2)
        return remote(
            out.at[dest],
            rows.at[u, b, a, pl.ds(i * cap, cap), :],
            z_send.at[j],
            z_recv.at[j],
            {"ep": dest},
        )

    def halo_copy(i):
        source = tokens if i == 0 else HALF_WIN
        target = 0 if i == 0 else HALF_WIN + tokens
        return remote(
            raw.at[pl.ds(source, HALF_WIN)],
            raw.at[pl.ds(target, HALF_WIN)],
            halo_send.at[i],
            halo_recv.at[i],
            {"ep": (ep + (1 if i == 0 else senders - 1)) % senders},
        )

    for j in range(1, 4):
        z_copy(j).start()
    for i in range(2):
        halo_copy(i).start()
    for j in range(4, senders):
        z_copy(j).start()
    a0, b0 = own_ab(0)
    rows[0, b0, a0, 0:cap, :] = out[ep]

    for load in loads[5:7]:
        load.wait()

    def turn_table(first, count):
        position = lax.broadcasted_iota(jnp.int32, (count, LANES), 0) + (first_row + first)
        angles = position.astype(F32) * freq_ref[...]
        return jnp.cos(angles), jnp.sin(angles)

    def rotate_keys(first, count, table):
        cosine, sine = table
        held = raw[HALF_WIN + first : HALF_WIN + first + count]
        turned = dot(held, selector(LANES, 0, 0, True))
        turned = held.astype(F32) * cosine + turned * sine
        ext[HALF_WIN + first : HALF_WIN + first + count] = turned.astype(BF16)

    table = turn_table(0, tokens)
    rotate_keys(0, tokens, table)

    def query_dot(turned):
        return lax.dot_general(
            query_ref[...],
            selector(HEAD_DIM, 0, 0, turned),
            (((0,), (0,)), ((), ())),
            preferred_element_type=F32,
        )

    rot_q[...] = (query_dot(False) * table[0] + query_dot(True) * table[1]).astype(BF16)

    def attend(i):
        if i == 0:
            halo_copy(0).wait_recv()
            rotate_keys(-HALF_WIN, HALF_WIN, turn_table(-HALF_WIN, HALF_WIN))
        if i == blocks - 1:
            halo_copy(1).wait_recv()
            rotate_keys(tokens, HALF_WIN, turn_table(tokens, HALF_WIN))
        near = 3 * HALF_WIN
        window = ext[i * HALF_WIN : i * HALF_WIN + near]
        block_q = rot_q[i * HALF_WIN : (i + 1) * HALF_WIN]
        scores = lax.dot_general(
            block_q, window, (((1,), (1,)), ((), ())), preferred_element_type=F32
        ) * HEAD_DIM ** (-0.5)
        shape = (HALF_WIN, near)
        q_at, k_at = (lax.broadcasted_iota(jnp.int32, shape, d) for d in range(2))
        gap = k_at - q_at
        global_key = first_row + (i - 1) * HALF_WIN + k_at
        allowed = (gap >= 0) & (gap <= 2 * HALF_WIN)
        allowed = allowed & (global_key >= 0) & (global_key < senders * tokens)
        scores = jnp.where(allowed, scores, NEG_BIG)
        sink = sink_ref[...]
        row_peak = jnp.maximum(jnp.max(scores, axis=1, keepdims=True), sink)
        lifted = jnp.exp(scores - row_peak)
        norm_total = jnp.sum(lifted, axis=1, keepdims=True) + jnp.exp(sink - row_peak)
        probs = (lifted / norm_total).astype(BF16)
        weighted = dot(probs, window)
        a, b = own_ab((i // 2) % 2)
        piece_cols = slice((i % 2) * HALF_WIN, (i % 2 + 1) * HALF_WIN)
        att[i // 2, b, a, :, piece_cols] = weighted.T[HEAD_DIM:].astype(BF16)

    def buffer(u):
        return (rows, u) if u < units else (att, u - units)

    def gather_a(u, k, back=False):
        par = u % 2
        a, b = own_ab(par)
        buf, at = buffer(u)
        return remote(
            buf.at[at, b, a],
            buf.at[at, b, (a + SIDE - k) % SIDE if back else a],
            ag_send.at[u, k - 1],
            ag_recv.at[u, k - 1],
            along_a(par, k),
        )

    def gather_b(u, k, s, back=False):
        par = u % 2
        a, b = own_ab(par)
        buf, at = buffer(u)
        col = (a + SIDE - k) % SIDE
        sem = 3 + 2 * k + (0 if s == 1 else 1)
        return remote(
            buf.at[at, b, col],
            buf.at[at, (b + SIDE - s) % SIDE if back else b, col],
            ag_send.at[u, sem],
            ag_recv.at[u, sem],
            along_b(par, s % SIDE),
        )

    def gather_c(u, k, back=False):
        par = u % 2
        a, b = own_ab(par)
        buf, at = buffer(u)
        s = RELAY[k]
        col = (a + SIDE - k) % SIDE
        held = (b + SIDE - s) % SIDE
        return remote(
            buf.at[at, held, col],
            buf.at[at, (b + 2) % SIDE if back else held, col],
            ag_send.at[u, 11 + k],
            ag_recv.at[u, 11 + k],
            along_b(par, s % SIDE),
        )

    turns = ((0, 1), (1, SIDE - 1))

    def reduce_opposite(u, i, k):
        par = u % 2
        a, b = own_ab(par)
        return remote(
            terms.at[u, (b + 2) % SIDE, pl.ds(2 * i, 2)],
            transit.at[u, i],
            rs_send.at[u, i],
            rs_recv.at[u, i],
            along_b(par, k),
        )

    def reduce_next(u, i, k):
        par = u % 2
        a, b = own_ab(par)
        rest = pl.ds(2 - 2 * i, 2)
        return remote(
            terms.at[u, (b + k) % SIDE, rest],
            from_b.at[u, i, rest],
            rs_send.at[u, 2 + i],
            rs_recv.at[u, 2 + i],
            along_b(par, k),
        )

    def reduce_relay(u, i, k):
        return remote(
            transit.at[u, i],
            from_b.at[u, i, pl.ds(2 * i, 2)],
            rs_send.at[u, 4 + i],
            rs_recv.at[u, 4 + i],
            along_b(u % 2, k),
        )

    def reduce_a(u, k):
        a, b = own_ab(u % 2)
        return remote(
            part.at[u, (a + k) % SIDE],
            from_a.at[u, k - 1],
            rs_send.at[u, 5 + k],
            rs_recv.at[u, 5 + k],
            along_a(u % 2, k),
        )

    def ret_copy(j):
        source = ep_plus(chips - distance(j), j % 2)
        return remote(
            result.at[j // PER_UNIT, pl.ds((j % PER_UNIT) * cap, cap), :],
            returned.at[ep],
            ret_send.at[j],
            ret_recv.at[j],
            {"ep": source},
        )

    def gathered(u):
        for k, s in RELAY.items():
            gather_b(u, k, -s, back=True).wait_recv()
            gather_c(u, k, back=True).wait_recv()
        buf, at = buffer(u)
        if u % 2 == 0:
            places = [(t // SIDE, t % SIDE) for t in range(SIDE * SIDE)]
        else:
            places = [(t % SIDE, t // SIDE) for t in range(SIDE * SIDE)]
        return places, [buf[(at, *place)] for place in places]

    loaded = []

    def expert(u):
        places, pieces = gathered(u)
        if not loaded:
            loaded.append(u)
            for load in loads[8:11]:
                load.wait()
        x = jnp.concatenate(pieces, axis=1)
        gate = dot(x, wg[...])
        up = dot(x, wu[...])
        hidden = (gate / (1.0 + jnp.exp(-gate)) * up).astype(BF16)
        for t, place in enumerate(places):
            terms[(u, *place)] = dot(hidden, wd[:, t * LANES : (t + 1) * LANES]).astype(BF16)
        for i, k in turns:
            reduce_opposite(u, i, k).start()
        for i, k in turns:
            reduce_next(u, i, k).start()

    projected = []

    def project(u):
        places, pieces = gathered(u)
        if not projected:
            loads[11].wait()
        projected.append(u)
        x = jnp.concatenate(pieces, axis=0)
        half = x.shape[1]
        at = (u - units) * half
        total = lax.dot_general(x, wo[...], (((0,), (0,)), ((), ())), preferred_element_type=F32)
        mixer_ref[at : at + half] = total.astype(BF16)

    for event in order:
        kind, u = event[:2]
        a, b = own_ab(u % 2)
        if kind == "Q":
            attend(u)
        elif kind == "A0":
            if u < units:
                for j in range(u * PER_UNIT, (u + 1) * PER_UNIT):
                    if j:
                        z_copy(j).wait_recv()
            for k in (1, 3, 2):
                gather_a(u, k).start()
            for s in (1, -1):
                gather_b(u, 0, s).start()
        elif kind == "A1":
            k = event[2]
            gather_a(u, k, back=True).wait_recv()
            for s in (1, -1):
                gather_b(u, k, s).start()
        elif kind == "A2":
            k = event[2]
            gather_b(u, k, RELAY[k], back=True).wait_recv()
            gather_c(u, k).start()
        elif kind == "C":
            expert(u)
        elif kind == "P":
            project(u)
        elif kind == "R1":
            i, k = turns[event[2]]
            reduce_opposite(u, i, k).wait_recv()
            held = terms[u, (b + k) % SIDE, 2 * i : 2 * i + 2]
            transit[u, i] = (transit[u, i].astype(F32) + held.astype(F32)).astype(BF16)
            reduce_relay(u, i, k).start()
        elif kind == "R2":
            for i, k in turns:
                reduce_next(u, i, k).wait_recv()
                reduce_relay(u, i, k).wait_recv()
            part[u] = (
                terms[u, b].astype(F32) + from_b[u, 0].astype(F32) + from_b[u, 1].astype(F32)
            ).astype(BF16)
            for k in (1, 3, 2):
                reduce_a(u, k).start()
        elif kind == "R3":
            total = part[u, a].astype(F32)
            for k in (1, 3, 2):
                reduce_a(u, k).wait_recv()
                total = total + from_a[u, k - 1].astype(F32)
            result[u] = total.astype(BF16)
            for j in range(u * PER_UNIT, (u + 1) * PER_UNIT):
                if j:
                    ret_copy(j).start()
                else:
                    returned[ep] = result[0, 0:cap, :]

    for u in range(units + 2):
        for k in (1, 3, 2):
            gather_a(u, k).wait_send()
        for k in range(SIDE):
            for s in (1, -1):
                gather_b(u, k, s).wait_send()
            gather_c(u, k).wait_send()
    for u in range(units):
        for i, k in turns:
            reduce_opposite(u, i, k).wait_send()
            reduce_next(u, i, k).wait_send()
            reduce_relay(u, i, k).wait_send()
        for k in (1, 3, 2):
            reduce_a(u, k).wait_send()
    for i in range(2):
        halo_copy(i).wait_send()
    for j in range(1, senders):
        z_copy(j).wait_send()
    loads[7].wait()
    weights = [upright(weights_ref[k : k + 1]) for k in range(TOP_K)]
    for j in range(1, senders):
        ret_copy(j).wait()
    back = returned[...].reshape(senders * cap, LANES)
    combined = dot(picks[0], back) * weights[0]
    combined = combined + dot(picks[1], back) * weights[1]
    expert_ref[...] = combined.astype(BF16)


def local(
    query_proj,
    key_proj,
    value_proj,
    sink_logit,
    out_weight,
    expert_input,
    norm_gain,
    routes,
    route_weights,
    gate_weight,
    up_weight,
    down_weight,
):
    row_count, width = expert_input.shape
    tokens = query_proj.shape[0]
    senders = gate_weight.shape[0] * lax.axis_size("ep")
    cap = row_count * GROUPS // senders
    units = senders // PER_UNIT
    steps = np.arange(HEAD_DIM // 2, dtype=np.float32) * np.float32(2.0 / HEAD_DIM)
    inverse_freq = np.float32(1.0) / np.float32(ROPE_BASE) ** steps
    zeros = np.zeros(LANES - HEAD_DIM, np.float32)
    freq = np.concatenate([inverse_freq, inverse_freq, zeros])[None, :]

    vmem = pl.BlockSpec(memory_space=pltpu.VMEM)
    hbm = pl.BlockSpec(memory_space=pl.ANY)
    dma = pltpu.SemaphoreType.DMA
    block = (PER_UNIT * cap, LANES)
    gate, up, down = gate_weight[0], up_weight[0], down_weight[0]
    operands = (
        expert_input,
        norm_gain[None, :],
        routes.T,
        key_proj,
        value_proj,
        query_proj.T,
        jnp.asarray(freq),
        route_weights.T,
        gate,
        up,
        down,
        out_weight,
    )
    return pl.pallas_call(
        functools.partial(layer_kernel, units, plan(units)),
        out_shape=(
            jax.ShapeDtypeStruct((tokens, LANES), BF16),
            jax.ShapeDtypeStruct((row_count, LANES), BF16),
        ),
        in_specs=[vmem] + [hbm] * len(operands),
        out_specs=(vmem, vmem),
        scratch_shapes=[
            pltpu.VMEM((senders, cap, LANES), BF16),
            pltpu.VMEM((TOP_K, row_count, senders * cap), BF16),
            pltpu.VMEM((tokens + 2 * HALF_WIN, LANES), BF16),
            pltpu.VMEM((tokens + 2 * HALF_WIN, LANES), BF16),
            pltpu.VMEM((tokens, LANES), BF16),
            pltpu.VMEM((2, SIDE, SIDE, HEAD_DIM, tokens // 2), BF16),
            pltpu.VMEM((senders, cap, LANES), BF16),
            pltpu.VMEM((units, SIDE, SIDE, *block), BF16),
            pltpu.VMEM((units, SIDE, SIDE, *block), BF16),
            pltpu.VMEM((units, 2, 2, *block), BF16),
            pltpu.VMEM((units, 2, SIDE, *block), BF16),
            pltpu.VMEM((units, SIDE, *block), BF16),
            pltpu.VMEM((units, SIDE - 1, *block), BF16),
            pltpu.VMEM((units, *block), BF16),
            *(pltpu.VMEM(x.shape, x.dtype) for x in operands),
            dma((len(operands),)),
            dma((2,)),
            dma((2,)),
            dma((senders,)),
            dma((senders,)),
            dma((senders,)),
            dma((senders,)),
            dma((units + 2, 15)),
            dma((units + 2, 15)),
            dma((units, 9)),
            dma((units, 9)),
        ],
        compiler_params=pltpu.CompilerParams(
            collective_id=0, has_side_effects=True, vmem_limit_bytes=56 * 1024 * 1024
        ),
    )(sink_logit.reshape(1, 1), *operands)


def solution(mesh):
    finer = Mesh(mesh.devices.reshape(mesh.shape["ep"], SIDE, SIDE), ("ep", "tp_0", "tp_1"))
    in_specs = (
        P("ep", TP),
        P("ep", None),
        P("ep", None),
        P(TP),
        P(None, TP),
        P("ep", None),
        P(),
        P("ep", None),
        P("ep", None),
        P("ep", None, TP),
        P("ep", None, TP),
        P("ep", TP, None),
    )
    out_specs = (P("ep", TP), P("ep", TP))
    return jax.shard_map(local, mesh=finer, in_specs=in_specs, out_specs=out_specs, check_vma=False)
```

```python
import functools

import jax
import jax.numpy as jnp
import numpy as np
from jax import lax
from jax.experimental import pallas as pl
from jax.experimental.pallas import tpu as pltpu
from jax.sharding import Mesh
from jax.sharding import PartitionSpec as P

HEADS = 16
KV_HEADS = 4
HEAD_DIM = 64
HALF_WIN = 128
GROUPS = 4
TOP_K = 2
NORM_EPS = 1e-06
ROPE_BASE = 10000.0
NEG_BIG = -1e30
TP = ("tp_0", "tp_1")
SIDE = 4
LANES = 128
PER_UNIT = 4
BF16 = jnp.bfloat16
F32 = jnp.float32
MESH = pl.DeviceIdType.MESH

Z_ORDER = (0, 2, 14, 3, 9, 7, 8, 10, 6, 11, 12, 5, 4, 13, 1, 15)
Z_ARRIVAL = (0, 13, 3, 4.5, 15, 14, 12.5, 10, 12.5, 9.5, 11.5, 12.6, 13, 13.2, 3, 13)
RELAY = {0: 1, 1: 1, 3: -1, 2: -1}


def plan(units):
    piece, rate, latency = 32.0, 45.56, 2.4
    cost = {"Q": 0.6, "A0": 0.08, "A1": 0.05, "A2": 0.04, "C": 1.0, "P": 0.5}
    cost.update({"R1": 0.15, "R2": 0.3, "R3": 0.25})
    stage = ("Q", "A0", "A1", "A2", "C", "P", "R1", "R2", "R3")
    free, arrival, pending = {}, {}, {}

    def send(now, lanes, size, token, extra=0.0):
        ends = []
        for lane in lanes:
            free[lane] = max(free.get(lane, 0.0), now) + size / rate
            ends.append(free[lane])
        arrival[token] = max(ends) + latency + extra

    per = PER_UNIT // 2
    for u in range(units):
        arrival[("z", u)] = max(Z_ARRIVAL[k] for k in Z_ORDER[u * per : u * per + per])
    for i, ready in enumerate((3.5, 0.0, 0.0, 3.5)):
        arrival[("q", i)] = ready
        pending[("Q", i)] = [("q", i)]
    for u in range(units + 2):
        att = u - units
        first = [("z", u)] if att < 0 else [("Q", 2 * att), ("Q", 2 * att + 1)]
        pending[("A0", u)] = first
        for k in (1, 3, 2):
            pending[("A1", u, k)] = [("a", u, k)]
        for k, s in RELAY.items():
            pending[("A2", u, k)] = [("b", u, k, s)]
        rest = [("b", u, k, s) for k in range(SIDE) for s in (1, -1)]
        rest += [("c", u, k) for k in range(SIDE)]
        pending[("C" if att < 0 else "P", u)] = rest
        if att < 0:
            for i in range(2):
                pending[("R1", u, i)] = [("t", u, i)]
            pending[("R2", u)] = [("f", u, i, j) for i in range(2) for j in range(2)]
            pending[("R3", u)] = [("g", u, k) for k in (1, 2, 3)]

    now, order = 0.0, []
    while pending:
        ready, later = [], []
        for event, needs in pending.items():
            if all(need in arrival for need in needs):
                at = max(arrival[need] for need in needs)
                if at <= now:
                    kind, u = event[0], event[1]
                    place = -1 if kind == "Q" or u >= units else u
                    late = stage.index(kind) >= 4
                    ready.append((late, place, -stage.index(kind), event))
                else:
                    later.append(at)
        if not ready:
            now = min(later)
            continue
        event = min(ready)[-1]
        del pending[event]
        order.append(event)
        kind, u = event[:2]
        now += cost[kind]
        a, b = ("x", "y") if u % 2 == 0 else ("y", "x")
        both = ((a, 1), (a, -1))
        if kind == "Q":
            arrival[event] = now
        elif kind == "A0":
            send(now, both[:1], piece, ("a", u, 1))
            send(now, both[1:], piece, ("a", u, 3))
            send(now, both, piece, ("a", u, 2), 0.7)
        if kind in ("A0", "A1"):
            k = 0 if kind == "A0" else event[2]
            for s in (1, -1):
                send(now, ((b, s),), piece, ("b", u, k, s))
        elif kind == "A2":
            send(now, ((b, RELAY[event[2]]),), piece, ("c", u, event[2]))
        elif kind == "C":
            for i, s in enumerate((1, -1)):
                send(now, ((b, s),), 2 * piece, ("t", u, i))
            for i, s in enumerate((1, -1)):
                send(now, ((b, s),), 2 * piece, ("f", u, i, 0))
        elif kind == "R1":
            send(now, ((b, 1 - 2 * event[2]),), 2 * piece, ("f", u, event[2], 1))
        elif kind == "R2":
            send(now, both[:1], piece, ("g", u, 1))
            send(now, both[1:], piece, ("g", u, 3))
            send(now, both, piece, ("g", u, 2), 0.7)
    return order


def layer_kernel(
    units,
    order,
    sink_ref,
    input_hbm,
    gain_hbm,
    routes_hbm,
    key_hbm,
    value_hbm,
    query_hbm,
    freq_hbm,
    weights_hbm,
    wg_hbm,
    wu_hbm,
    wd_hbm,
    wo_hbm,
    mixer_ref,
    expert_ref,
    out,
    picks,
    raw,
    ext,
    rot_q,
    att,
    returned,
    rows,
    terms,
    transit,
    from_b,
    part,
    from_a,
    result,
    input_ref,
    gain_ref,
    routes_ref,
    key_ref,
    value_ref,
    query_ref,
    freq_ref,
    weights_ref,
    wg,
    wu,
    wd,
    wo,
    load_sem,
    halo_send,
    halo_recv,
    z_send,
    z_recv,
    ret_send,
    ret_recv,
    ag_send,
    ag_recv,
    rs_send,
    rs_recv,
):
    ep = lax.axis_index("ep")
    yi = lax.axis_index("tp_0")
    xi = lax.axis_index("tp_1")
    tp = yi * SIDE + xi
    senders = units * PER_UNIT
    chips = senders // 2
    zi = ep // 2
    ci = ep % 2
    cap = out.shape[1]
    tokens = query_ref.shape[1]
    blocks = tokens // HALF_WIN

    def distance(j):
        return Z_ORDER[j // 2]

    def ep_plus(step, flip):
        return ((zi + step) % chips) * 2 + (ci + flip) % 2

    def along_a(par, k):
        return {"tp_0": (yi + k * par) % SIDE, "tp_1": (xi + k * (1 - par)) % SIDE}

    def along_b(par, k):
        return along_a(1 - par, k)

    def own_ab(par):
        return (xi, yi) if par == 0 else (yi, xi)

    def remote(src, dst, ssem, rsem, dev):
        return pltpu.make_async_remote_copy(
            src_ref=src,
            dst_ref=dst,
            send_sem=ssem,
            recv_sem=rsem,
            device_id=dev,
            device_id_type=MESH,
        )

    barrier = pltpu.get_barrier_semaphore()
    for j in range(1, senders):
        pl.semaphore_signal(
            barrier, inc=1, device_id={"ep": ep_plus(j // 2, j % 2)}, device_id_type=MESH
        )
    for par in range(2):
        for k in range(1, SIDE):
            pl.semaphore_signal(barrier, inc=1, device_id=along_a(par, k), device_id_type=MESH)

    to_load = (
        (input_hbm, input_ref),
        (gain_hbm, gain_ref),
        (routes_hbm, routes_ref),
        (key_hbm, key_ref),
        (value_hbm, value_ref),
        (query_hbm, query_ref),
        (freq_hbm, freq_ref),
        (weights_hbm, weights_ref),
        (wg_hbm, wg),
        (wu_hbm, wu),
        (wd_hbm, wd),
        (wo_hbm, wo),
    )
    loads = [pltpu.make_async_copy(s, d, load_sem.at[i]) for i, (s, d) in enumerate(to_load)]
    for load in loads:
        load.start()

    def upright(row):
        return jnp.broadcast_to(row, (LANES, row.shape[1])).T

    row_count = input_ref.shape[0]
    for load in loads[:3]:
        load.wait()
    widened = input_ref[...].astype(F32)
    scale = lax.rsqrt(jnp.mean(widened * widened, axis=1, keepdims=True) + NORM_EPS)
    cols = pl.ds(pl.multiple_of(tp * LANES, LANES), LANES)
    normed = (input_ref[:, cols].astype(F32) * scale * gain_ref[:, cols]).astype(BF16)
    routes = routes_ref[...].astype(F32)
    named_by = [upright(routes[k : k + 1]) for k in range(TOP_K)]
    lane = lax.broadcasted_iota(jnp.int32, (row_count, LANES), 1).astype(F32)
    hot = [named_by[k] == lane for k in range(TOP_K)]
    named = jnp.where(hot[0] | hot[1], 1.0, 0.0).astype(BF16)
    square = (row_count, row_count)
    down, across = (lax.broadcasted_iota(jnp.int32, square, d) for d in range(2))
    earlier = jnp.where(across < down, 1.0, 0.0).astype(BF16)
    before = jnp.dot(earlier, named, preferred_element_type=F32)
    slot_ids = lax.broadcasted_iota(jnp.int32, (row_count, senders * cap), 1)
    for k in range(TOP_K):
        rank = jnp.sum(jnp.where(hot[k], before, 0.0), axis=1, keepdims=True)
        slot = (named_by[k][:, 0:1] * cap + rank).astype(jnp.int32)
        picks[k] = jnp.where(slot == slot_ids, 1.0, 0.0).astype(BF16)
    placed = picks[0] + picks[1]
    outgoing = lax.dot_general(
        placed, normed, (((0,), (0,)), ((), ())), preferred_element_type=F32
    )
    out[...] = outgoing.astype(BF16).reshape(senders, cap, LANES)

    first_row = ep * tokens

    def selector(depth, first, target, turned):
        shape = (depth, LANES)
        r, c = (lax.broadcasted_iota(jnp.int32, shape, d) for d in range(2))
        inside = (c >= target) & (c < target + HEAD_DIM)
        at = first + c - target
        if not turned:
            return jnp.where(inside & (r == at), 1.0, 0.0).astype(BF16)
        low = c < HEAD_DIM // 2
        half = HEAD_DIM // 2
        sign = jnp.where(low & (r == at + half), -1.0, 0.0)
        sign = sign + jnp.where(~low & (r == at - half), 1.0, 0.0)
        return jnp.where(inside, sign, 0.0).astype(BF16)

    def dot(a, b):
        return jnp.dot(a, b, preferred_element_type=F32)

    for load in loads[3:5]:
        load.wait()
    depth = key_ref.shape[1]
    own = (tp // (HEADS // KV_HEADS)) * HEAD_DIM
    plain = dot(key_ref[...], selector(depth, own, 0, False))
    plain = plain + dot(value_ref[...], selector(depth, own, HEAD_DIM, False))
    raw[HALF_WIN : HALF_WIN + tokens] = plain.astype(BF16)

    pl.semaphore_wait(barrier, senders - 1 + 2 * (SIDE - 1))

    def z_copy(j):
        u, i = j // PER_UNIT, j % PER_UNIT
        a, b = own_ab(u % 2)
        dest = ep_plus(distance(j), j % 2)
        return remote(
            out.at[dest],
            rows.at[u, b, a, pl.ds(i * cap, cap), :],
            z_send.at[j],
            z_recv.at[j],
            {"ep": dest},
        )

    def halo_copy(i):
        source = tokens if i == 0 else HALF_WIN
        target = 0 if i == 0 else HALF_WIN + tokens
        return remote(
            raw.at[pl.ds(source, HALF_WIN)],
            raw.at[pl.ds(target, HALF_WIN)],
            halo_send.at[i],
            halo_recv.at[i],
            {"ep": (ep + (1 if i == 0 else senders - 1)) % senders},
        )

    for j in range(1, 4):
        z_copy(j).start()
    for i in range(2):
        halo_copy(i).start()
    for j in range(4, senders):
        z_copy(j).start()
    a0, b0 = own_ab(0)
    rows[0, b0, a0, 0:cap, :] = out[ep]

    for load in loads[5:7]:
        load.wait()

    def turn_table(first, count):
        position = lax.broadcasted_iota(jnp.int32, (count, LANES), 0) + (first_row + first)
        angles = position.astype(F32) * freq_ref[...]
        return jnp.cos(angles), jnp.sin(angles)

    def rotate_keys(first, count, table):
        cosine, sine = table
        held = raw[HALF_WIN + first : HALF_WIN + first + count]
        turned = dot(held, selector(LANES, 0, 0, True))
        turned = held.astype(F32) * cosine + turned * sine
        ext[HALF_WIN + first : HALF_WIN + first + count] = turned.astype(BF16)

    table = turn_table(0, tokens)
    rotate_keys(0, tokens, table)

    def query_dot(turned):
        return lax.dot_general(
            query_ref[...],
            selector(HEAD_DIM, 0, 0, turned),
            (((0,), (0,)), ((), ())),
            preferred_element_type=F32,
        )

    rot_q[...] = (query_dot(False) * table[0] + query_dot(True) * table[1]).astype(BF16)

    def attend(i):
        if i == 0:
            halo_copy(0).wait_recv()
            rotate_keys(-HALF_WIN, HALF_WIN, turn_table(-HALF_WIN, HALF_WIN))
        if i == blocks - 1:
            halo_copy(1).wait_recv()
            rotate_keys(tokens, HALF_WIN, turn_table(tokens, HALF_WIN))
        near = 3 * HALF_WIN
        window = ext[i * HALF_WIN : i * HALF_WIN + near]
        block_q = rot_q[i * HALF_WIN : (i + 1) * HALF_WIN]
        scores = lax.dot_general(
            block_q, window, (((1,), (1,)), ((), ())), preferred_element_type=F32
        ) * HEAD_DIM ** (-0.5)
        shape = (HALF_WIN, near)
        q_at, k_at = (lax.broadcasted_iota(jnp.int32, shape, d) for d in range(2))
        gap = k_at - q_at
        global_key = first_row + (i - 1) * HALF_WIN + k_at
        allowed = (gap >= 0) & (gap <= 2 * HALF_WIN)
        allowed = allowed & (global_key >= 0) & (global_key < senders * tokens)
        scores = jnp.where(allowed, scores, NEG_BIG)
        sink = sink_ref[...]
        row_peak = jnp.maximum(jnp.max(scores, axis=1, keepdims=True), sink)
        lifted = jnp.exp(scores - row_peak)
        norm_total = jnp.sum(lifted, axis=1, keepdims=True) + jnp.exp(sink - row_peak)
        probs = (lifted / norm_total).astype(BF16)
        weighted = dot(probs, window)
        a, b = own_ab((i // 2) % 2)
        piece_cols = slice((i % 2) * HALF_WIN, (i % 2 + 1) * HALF_WIN)
        att[i // 2, b, a, :, piece_cols] = weighted.T[HEAD_DIM:].astype(BF16)

    def buffer(u):
        return (rows, u) if u < units else (att, u - units)

    def gather_a(u, k, back=False):
        par = u % 2
        a, b = own_ab(par)
        buf, at = buffer(u)
        return remote(
            buf.at[at, b, a],
            buf.at[at, b, (a + SIDE - k) % SIDE if back else a],
            ag_send.at[u, k - 1],
            ag_recv.at[u, k - 1],
            along_a(par, k),
        )

    def gather_b(u, k, s, back=False):
        par = u % 2
        a, b = own_ab(par)
        buf, at = buffer(u)
        col = (a + SIDE - k) % SIDE
        sem = 3 + 2 * k + (0 if s == 1 else 1)
        return remote(
            buf.at[at, b, col],
            buf.at[at, (b + SIDE - s) % SIDE if back else b, col],
            ag_send.at[u, sem],
            ag_recv.at[u, sem],
            along_b(par, s % SIDE),
        )

    def gather_c(u, k, back=False):
        par = u % 2
        a, b = own_ab(par)
        buf, at = buffer(u)
        s = RELAY[k]
        col = (a + SIDE - k) % SIDE
        held = (b + SIDE - s) % SIDE
        return remote(
            buf.at[at, held, col],
            buf.at[at, (b + 2) % SIDE if back else held, col],
            ag_send.at[u, 11 + k],
            ag_recv.at[u, 11 + k],
            along_b(par, s % SIDE),
        )

    turns = ((0, 1), (1, SIDE - 1))

    def reduce_opposite(u, i, k):
        par = u % 2
        a, b = own_ab(par)
        return remote(
            terms.at[u, (b + 2) % SIDE, pl.ds(2 * i, 2)],
            transit.at[u, i],
            rs_send.at[u, i],
            rs_recv.at[u, i],
            along_b(par, k),
        )

    def reduce_next(u, i, k):
        par = u % 2
        a, b = own_ab(par)
        rest = pl.ds(2 - 2 * i, 2)
        return remote(
            terms.at[u, (b + k) % SIDE, rest],
            from_b.at[u, i, rest],
            rs_send.at[u, 2 + i],
            rs_recv.at[u, 2 + i],
            along_b(par, k),
        )

    def reduce_relay(u, i, k):
        return remote(
            transit.at[u, i],
            from_b.at[u, i, pl.ds(2 * i, 2)],
            rs_send.at[u, 4 + i],
            rs_recv.at[u, 4 + i],
            along_b(u % 2, k),
        )

    def reduce_a(u, k):
        a, b = own_ab(u % 2)
        return remote(
            part.at[u, (a + k) % SIDE],
            from_a.at[u, k - 1],
            rs_send.at[u, 5 + k],
            rs_recv.at[u, 5 + k],
            along_a(u % 2, k),
        )

    def ret_copy(j):
        source = ep_plus(chips - distance(j), j % 2)
        return remote(
            result.at[j // PER_UNIT, pl.ds((j % PER_UNIT) * cap, cap), :],
            returned.at[ep],
            ret_send.at[j],
            ret_recv.at[j],
            {"ep": source},
        )

    def gathered(u):
        for k, s in RELAY.items():
            gather_b(u, k, -s, back=True).wait_recv()
            gather_c(u, k, back=True).wait_recv()
        buf, at = buffer(u)
        if u % 2 == 0:
            places = [(t // SIDE, t % SIDE) for t in range(SIDE * SIDE)]
        else:
            places = [(t % SIDE, t // SIDE) for t in range(SIDE * SIDE)]
        return places, [buf[(at, *place)] for place in places]

    loaded = []

    def expert(u):
        places, pieces = gathered(u)
        if not loaded:
            loaded.append(u)
            for load in loads[8:11]:
                load.wait()
        x = jnp.concatenate(pieces, axis=1)
        gate = dot(x, wg[...])
        up = dot(x, wu[...])
        hidden = (gate / (1.0 + jnp.exp(-gate)) * up).astype(BF16)
        for t, place in enumerate(places):
            terms[(u, *place)] = dot(hidden, wd[:, t * LANES : (t + 1) * LANES]).astype(BF16)
        for i, k in turns:
            reduce_opposite(u, i, k).start()
        for i, k in turns:
            reduce_next(u, i, k).start()

    projected = []

    def project(u):
        places, pieces = gathered(u)
        if not projected:
            loads[11].wait()
        projected.append(u)
        x = jnp.concatenate(pieces, axis=0)
        half = x.shape[1]
        at = (u - units) * half
        total = lax.dot_general(x, wo[...], (((0,), (0,)), ((), ())), preferred_element_type=F32)
        mixer_ref[at : at + half] = total.astype(BF16)

    for event in order:
        kind, u = event[:2]
        a, b = own_ab(u % 2)
        if kind == "Q":
            attend(u)
        elif kind == "A0":
            if u < units:
                for j in range(u * PER_UNIT, (u + 1) * PER_UNIT):
                    if j:
                        z_copy(j).wait_recv()
            for k in (1, 3, 2):
                gather_a(u, k).start()
            for s in (1, -1):
                gather_b(u, 0, s).start()
        elif kind == "A1":
            k = event[2]
            gather_a(u, k, back=True).wait_recv()
            for s in (1, -1):
                gather_b(u, k, s).start()
        elif kind == "A2":
            k = event[2]
            gather_b(u, k, RELAY[k], back=True).wait_recv()
            gather_c(u, k).start()
        elif kind == "C":
            expert(u)
        elif kind == "P":
            project(u)
        elif kind == "R1":
            i, k = turns[event[2]]
            reduce_opposite(u, i, k).wait_recv()
            held = terms[u, (b + k) % SIDE, 2 * i : 2 * i + 2]
            transit[u, i] = (transit[u, i].astype(F32) + held.astype(F32)).astype(BF16)
            reduce_relay(u, i, k).start()
        elif kind == "R2":
            for i, k in turns:
                reduce_next(u, i, k).wait_recv()
                reduce_relay(u, i, k).wait_recv()
            part[u] = (
                terms[u, b].astype(F32) + from_b[u, 0].astype(F32) + from_b[u, 1].astype(F32)
            ).astype(BF16)
            for k in (1, 3, 2):
                reduce_a(u, k).start()
        elif kind == "R3":
            total = part[u, a].astype(F32)
            for k in (1, 3, 2):
                reduce_a(u, k).wait_recv()
                total = total + from_a[u, k - 1].astype(F32)
            result[u] = total.astype(BF16)
            for j in range(u * PER_UNIT, (u + 1) * PER_UNIT):
                if j:
                    ret_copy(j).start()
                else:
                    returned[ep] = result[0, 0:cap, :]

    for u in range(units + 2):
        for k in (1, 3, 2):
            gather_a(u, k).wait_send()
        for k in range(SIDE):
            for s in (1, -1):
                gather_b(u, k, s).wait_send()
            gather_c(u, k).wait_send()
    for u in range(units):
        for i, k in turns:
            reduce_opposite(u, i, k).wait_send()
            reduce_next(u, i, k).wait_send()
            reduce_relay(u, i, k).wait_send()
        for k in (1, 3, 2):
            reduce_a(u, k).wait_send()
    for i in range(2):
        halo_copy(i).wait_send()
    for j in range(1, senders):
        z_copy(j).wait_send()
    loads[7].wait()
    weights = [upright(weights_ref[k : k + 1]) for k in range(TOP_K)]
    for j in range(1, senders):
        ret_copy(j).wait()
    back = returned[...].reshape(senders * cap, LANES)
    combined = dot(picks[0], back) * weights[0]
    combined = combined + dot(picks[1], back) * weights[1]
    expert_ref[...] = combined.astype(BF16)


def local(
    query_proj,
    key_proj,
    value_proj,
    sink_logit,
    out_weight,
    expert_input,
    norm_gain,
    routes,
    route_weights,
    gate_weight,
    up_weight,
    down_weight,
):
    row_count, width = expert_input.shape
    tokens = query_proj.shape[0]
    senders = gate_weight.shape[0] * lax.axis_size("ep")
    cap = row_count * GROUPS // senders
    units = senders // PER_UNIT
    steps = np.arange(HEAD_DIM // 2, dtype=np.float32) * np.float32(2.0 / HEAD_DIM)
    inverse_freq = np.float32(1.0) / np.float32(ROPE_BASE) ** steps
    zeros = np.zeros(LANES - HEAD_DIM, np.float32)
    freq = np.concatenate([inverse_freq, inverse_freq, zeros])[None, :]

    vmem = pl.BlockSpec(memory_space=pltpu.VMEM)
    hbm = pl.BlockSpec(memory_space=pl.ANY)
    dma = pltpu.SemaphoreType.DMA
    block = (PER_UNIT * cap, LANES)
    gate, up, down = gate_weight[0], up_weight[0], down_weight[0]
    operands = (
        expert_input,
        norm_gain[None, :],
        routes.T,
        key_proj,
        value_proj,
        query_proj.T,
        jnp.asarray(freq),
        route_weights.T,
        gate,
        up,
        down,
        out_weight,
    )
    return pl.pallas_call(
        functools.partial(layer_kernel, units, plan(units)),
        out_shape=(
            jax.ShapeDtypeStruct((tokens, LANES), BF16),
            jax.ShapeDtypeStruct((row_count, LANES), BF16),
        ),
        in_specs=[vmem] + [hbm] * len(operands),
        out_specs=(vmem, vmem),
        scratch_shapes=[
            pltpu.VMEM((senders, cap, LANES), BF16),
            pltpu.VMEM((TOP_K, row_count, senders * cap), BF16),
            pltpu.VMEM((tokens + 2 * HALF_WIN, LANES), BF16),
            pltpu.VMEM((tokens + 2 * HALF_WIN, LANES), BF16),
            pltpu.VMEM((tokens, LANES), BF16),
            pltpu.VMEM((2, SIDE, SIDE, HEAD_DIM, tokens // 2), BF16),
            pltpu.VMEM((senders, cap, LANES), BF16),
            pltpu.VMEM((units, SIDE, SIDE, *block), BF16),
            pltpu.VMEM((units, SIDE, SIDE, *block), BF16),
            pltpu.VMEM((units, 2, 2, *block), BF16),
            pltpu.VMEM((units, 2, SIDE, *block), BF16),
            pltpu.VMEM((units, SIDE, *block), BF16),
            pltpu.VMEM((units, SIDE - 1, *block), BF16),
            pltpu.VMEM((units, *block), BF16),
            *(pltpu.VMEM(x.shape, x.dtype) for x in operands),
            dma((len(operands),)),
            dma((2,)),
            dma((2,)),
            dma((senders,)),
            dma((senders,)),
            dma((senders,)),
            dma((senders,)),
            dma((units + 2, 15)),
            dma((units + 2, 15)),
            dma((units, 9)),
            dma((units, 9)),
        ],
        compiler_params=pltpu.CompilerParams(
            collective_id=0, has_side_effects=True, vmem_limit_bytes=56 * 1024 * 1024
        ),
    )(sink_logit.reshape(1, 1), *operands)


def solution(mesh):
    finer = Mesh(mesh.devices.reshape(mesh.shape["ep"], SIDE, SIDE), ("ep", "tp_0", "tp_1"))
    in_specs = (
        P("ep", TP),
        P("ep", None),
        P("ep", None),
        P(TP),
        P(None, TP),
        P("ep", None),
        P(),
        P("ep", None),
        P("ep", None),
        P("ep", None, TP),
        P("ep", None, TP),
        P("ep", TP, None),
    )
    out_specs = (P("ep", TP), P("ep", TP))
    return jax.shard_map(local, mesh=finer, in_specs=in_specs, out_specs=out_specs, check_vma=False)
```
